256 devices in a mesh: grp: 2 (over y), sp: 16 (over z), tp: 8 (over x, core).
Axes of the slice: x: 4, y: 2, z: 16, core: 2. Of those that a mesh axis runs over, the one named last changes fastest.
The devices are a block of a 4x16x16 slice.
Arguments:
- layer_feed: bfloat16 [4, 8192, 4096], P('grp', 'sp'), parts along dimension 0, may hold values from -13 to 13
- address_mapping: bfloat16 [4096, 2048], P(None, 'tp'), may hold values from -0.09375 to 0.09375
- content_mapping: bfloat16 [4096, 2048], P(None, 'tp'), may hold values from -0.09375 to 0.09375
- beta_mapping_matrix: bfloat16 [4096, 32], replicated, may hold values from -0.032958984 to 0.029541016
- forgetting_mapping: bfloat16 [4096, 32], replicated, may hold values from -0.09375 to 0.09375
- logged_fading_speed: float32 [32], P('tp'), may hold values from -12 to -2.8
- extra_forgetting: bfloat16 [4, 8192, 32], P('grp', 'sp', 'tp'), parts along dimension 0, may hold values from -1.4 to 0
- opening_probe: bfloat16 [4, 2048], P('grp', 'tp'), parts along dimension 0, may hold values from -6 to 6
Outputs:
- context_memory_tensor: bfloat16 [4, 32, 64, 64], P('grp', 'tp', 'sp'), parts along dimension 0
- opening_normed_output: bfloat16 [4, 2048], P('grp', 'tp'), parts along dimension 0
The draws below stay inside these ranges and needn't reach their ends.
There are 2 independent parts, one for each index of `grp`. The reference program is written for one: setup_inputs(seed, part) draws one part's arguments, and reference() takes and returns one part's arrays. A program takes and returns all parts, laid end to end along the dimension named above; an argument that names none is the same for every part. Nothing has to cross between parts.
All inputs are finite; a program needn't handle non-finite values.
Results may differ from the reference program's by a relative error of at most 0.014.
Values sent between devices are 32-bit elements; how exact they have to be, the bound alone decides.
A program may use at most 64 MiB of HBM per device.

```python
import math
import jax
import jax.numpy as jnp
from jax import lax

D = 4096
H = 32
HEAD = 64
SEQS = 2
TOK_DEV = 1024
LEN = 8192


def draw_layer_feed(key, part):
    span = TOK_DEV // SEQS
    count = LEN // span
    normal_key = jax.random.fold_in(key, 11)
    scale_key = jax.random.fold_in(key, 12)
    shift_key = jax.random.fold_in(key, 13)
    base = jnp.clip(jax.random.normal(normal_key, (SEQS, count, span, D), jnp.float32), -4.0, 4.0)
    levels = jnp.exp(jax.random.uniform(scale_key, (SEQS, count, 1, 1), jnp.float32, math.log(0.3), math.log(3.0)))
    shifts = jax.random.uniform(shift_key, (SEQS, 1, 1, 1), jnp.float32, 0.45, 0.55)
    scaled = base * levels + shifts
    return scaled.reshape(SEQS, LEN, D).astype(jnp.bfloat16)


def draw_beta_mapping_matrix(key, part):
    noise_key = jax.random.fold_in(key, 41)
    noise = jnp.clip(jax.random.normal(noise_key, (D, H), jnp.float32), -4.0, 4.0) * 0.5
    return (noise * D ** (-0.5) - 7.0 / D).astype(jnp.bfloat16)


def draw_logged_fading_speed(key, part):
    pick_key = jax.random.fold_in(key, 21)
    slow_key = jax.random.fold_in(key, 22)
    fast_key = jax.random.fold_in(key, 23)
    fast = jax.random.bernoulli(pick_key, 0.5, (H,))
    slow_rate = jax.random.uniform(slow_key, (H,), jnp.float32, 0.1, 0.5) / LEN
    fast_rate = jnp.exp(jax.random.uniform(fast_key, (H,), jnp.float32, math.log(0.03), math.log(0.06)))
    return jnp.log(jnp.where(fast, fast_rate, slow_rate)).astype(jnp.float32)


def draw_extra_forgetting(key, part):
    place_key = jax.random.fold_in(key, 31)
    depth_key = jax.random.fold_in(key, 32)
    spots = jax.random.randint(place_key, (SEQS, 2, 1, H), 0, LEN)
    depths = jnp.log(jax.random.uniform(depth_key, (SEQS, 2, 1, H), jnp.float32, 0.5, 0.8))
    positions = jnp.arange(LEN)[None, None, :, None]
    total = jnp.sum(jnp.where(positions == spots, depths, 0.0), axis=1)
    return total.astype(jnp.bfloat16)


def block_scale(stream_key, shape, cuts, low, top_value):
    loudness = 1.0
    for position, blocks in cuts:
        heights = jax.random.uniform(jax.random.fold_in(jax.random.fold_in(stream_key, 6), position), (blocks,), jnp.float32, low / len(cuts), top_value / len(cuts))
        loudness = loudness * jnp.repeat(jnp.exp(heights), shape[position] // blocks).reshape((-1,) + (1,) * (len(shape) - 1 - position))
    return loudness


def centred(rng, shape, spread, reach, shards=(), held_as=jnp.bfloat16):
    array = spread * jax.random.normal(rng, shape, jnp.float32)
    if shards:
        array = array * block_scale(rng, shape, shards, -0.22, 0.18)
    return jnp.clip(array, -reach, reach).astype(held_as)


def setup_inputs(seed: int = 0, part: int = 0) -> dict:
    streams_of = jax.random.split(jax.random.key(seed), 9)
    part_keys = jax.random.split(jax.random.fold_in(streams_of[8], part), 9)
    layer_feed = draw_layer_feed(jax.random.fold_in(jax.random.fold_in(streams_of[8], part), 71), part)
    address_mapping = centred(streams_of[1], (D, H * HEAD), D ** -0.5, 0.09375, ((1, 8),))
    content_mapping = centred(streams_of[2], (D, H * HEAD), D ** -0.5, 0.09375, ((1, 8),))
    beta_mapping_matrix = draw_beta_mapping_matrix(jax.random.fold_in(streams_of[8], 71), part)
    forgetting_mapping = centred(streams_of[4], (D, H), D ** -0.5, 0.09375)
    logged_fading_speed = draw_logged_fading_speed(jax.random.fold_in(streams_of[8], 71), part)
    extra_forgetting = draw_extra_forgetting(jax.random.fold_in(jax.random.fold_in(streams_of[8], part), 71), part)
    opening_probe = centred(part_keys[7], (SEQS, H * HEAD), 1.0, 6.0, ((1, 8),))
    return dict(layer_feed=layer_feed, address_mapping=address_mapping, content_mapping=content_mapping, beta_mapping_matrix=beta_mapping_matrix, forgetting_mapping=forgetting_mapping, logged_fading_speed=logged_fading_speed, extra_forgetting=extra_forgetting, opening_probe=opening_probe)


def reference(layer_feed, address_mapping, content_mapping, beta_mapping_matrix, forgetting_mapping, logged_fading_speed, extra_forgetting, opening_probe):

    def lone_example(input_tokens):
        sequence_tokens, sequence_batch, sequence_query = input_tokens
        address_embeddings = jnp.dot(sequence_tokens, address_mapping, preferred_element_type=jnp.float32).astype(jnp.bfloat16)
        content_embeddings = jnp.dot(sequence_tokens, content_mapping, preferred_element_type=jnp.float32).astype(jnp.bfloat16)
        beta_raw_scores = jnp.dot(sequence_tokens, beta_mapping_matrix, preferred_element_type=jnp.float32).astype(jnp.bfloat16)
        forgetting_raw_scores = jnp.dot(sequence_tokens, forgetting_mapping, preferred_element_type=jnp.float32).astype(jnp.bfloat16)
        keys = jax.nn.silu(address_embeddings.astype(jnp.float32)).reshape(-1, H, HEAD)
        keys = keys * lax.rsqrt(lax.optimization_barrier(jnp.sum(keys * keys, axis=-1, keepdims=True)) + 1e-06)
        values = jax.nn.silu(content_embeddings.astype(jnp.float32)).reshape(-1, H, HEAD)
        betas = jax.nn.sigmoid(beta_raw_scores.astype(jnp.float32))
        decay_factors = -jnp.exp(logged_fading_speed) * jax.nn.softplus(forgetting_raw_scores.astype(jnp.float32)) + sequence_batch.astype(jnp.float32)

        def advance(state, items):
            key_vector_row, value_row, beta_row, gamma_row = items
            retained = jnp.exp(gamma_row)[:, None, None] * state
            estimate = jnp.einsum('yz,yzt->yt', key_vector_row, retained, precision=lax.Precision.HIGHEST)
            state = retained + (beta_row[:, None] * key_vector_row)[:, :, None] * (value_row - estimate)[:, None, :]
            return (state, None)
        start = jnp.zeros((H, HEAD, HEAD), jnp.float32)
        final, _ = lax.scan(advance, start, (keys, values, betas, decay_factors))
        state_store = final.astype(jnp.bfloat16)
        query_per_head = sequence_query.astype(jnp.float32).reshape(H, HEAD)
        state_readout = jnp.einsum('yz,yzt->yt', query_per_head, final, precision=lax.Precision.HIGHEST)
        state_readout = state_readout * lax.rsqrt(lax.optimization_barrier(jnp.mean(state_readout * state_readout, axis=-1, keepdims=True)) + 1e-06)
        return (state_store, state_readout.reshape(H * HEAD).astype(jnp.bfloat16))
    context_memory_tensor, opening_normed_output = lax.map(lone_example, (layer_feed, extra_forgetting, opening_probe))
    return (context_memory_tensor, opening_normed_output)
```

```python
import functools

import jax
import jax.numpy as jnp
from jax import lax
from jax.experimental import pallas as pl
from jax.experimental.pallas import tpu as pltpu
from jax.sharding import PartitionSpec as P

HEAD = 64
LANES = 128
CHUNK = 128
ROWS = 256
MESH = pl.DeviceIdType.MESH
F32 = jnp.float32
BF16 = jnp.bfloat16
NN = (((1,), (0,)), ((), ()))
NT = (((1,), (1,)), ((), ()))
TN = (((0,), (0,)), ((), ()))


def dot(left, right, dims=NN):
    return lax.dot_general(left, right, dims, preferred_element_type=F32)


def split(x):
    high = x.astype(BF16)
    return high, (x - high.astype(F32)).astype(BF16)


def matmul(left, right):
    lh, ll = split(left)
    rh, rl = split(right)
    wide = jnp.concatenate(
        [jnp.concatenate([rh, rl], axis=1), jnp.concatenate([rh, jnp.zeros_like(rh)], axis=1)], axis=0
    )
    both = dot(jnp.concatenate([lh, ll], axis=1), wide)
    return both[:, : right.shape[1]] + both[:, right.shape[1] :]


def iotas(shape):
    return lax.broadcasted_iota(jnp.int32, shape, 0), lax.broadcasted_iota(jnp.int32, shape, 1)


def swapped(x):
    return pltpu.roll(x, HEAD, 1)


def composed(later, earlier):
    i, j = iotas(later.shape)
    diagonal = (i < HEAD) == (j < HEAD)
    transfer = jnp.where(diagonal, swapped(later), 0.0)
    return matmul(transfer, earlier) + jnp.where(diagonal, later, 0.0)


def silu(x):
    return x / (1.0 + jnp.exp(-x))


def project(step, heads, all_heads, x_ref, w_ref, wg_ref, extra_ref, speed_ref, keys_ref, values_ref, cols_ref, turned_ref):
    rows = pl.ds(pl.multiple_of(step * ROWS, ROWS), ROWS)
    x = x_ref[rows, :]
    width = heads * HEAD
    both = dot(x, w_ref[...]).astype(BF16).astype(F32)
    gates = dot(x, wg_ref[...]).astype(BF16)
    keys = silu(both[:, :width])
    high, low = split(keys * keys)
    i, j = iotas((width, width))
    same = jnp.where(i // HEAD == j // HEAD, 1.0, 0.0).astype(BF16)
    squares = dot(high, same) + dot(low, same)
    keys_ref[rows, :] = keys * lax.rsqrt(squares + 1e-06)
    values_ref[rows, :] = silu(both[:, width:])

    first = lax.axis_index("tp") * heads
    i, j = iotas((LANES, LANES))
    taken = ((j < heads) & (i == first + j)) | (
        (j >= heads) & (j < 2 * heads) & (i == all_heads + first + j - heads)
    )
    pre = dot(gates, jnp.where(taken, 1.0, 0.0).astype(BF16))
    i, j = iotas((heads, LANES))
    extra = dot(extra_ref[rows, :], jnp.where(j == i + heads, 1.0, 0.0).astype(BF16))
    _, lane = iotas((1, LANES))
    speed = jnp.zeros((1, LANES), F32)
    for h in range(heads):
        speed = jnp.where(lane == heads + h, speed_ref[h], speed)
    beta = 1.0 / (1.0 + jnp.exp(-pre))
    plus = jnp.maximum(pre, 0.0) + jnp.log(1.0 + jnp.exp(-jnp.abs(pre)))
    decay = -jnp.exp(speed) * plus + extra
    i, j = iotas((CHUNK, CHUNK))
    until = jnp.where(i >= j, 1.0, 0.0)
    for part in range(ROWS // CHUNK):
        at = slice(part * CHUNK, (part + 1) * CHUNK)
        total = lax.dot_general(until, decay[at], NN, precision=lax.Precision.HIGHEST, preferred_element_type=F32)
        _, lane = iotas((CHUNK, LANES))
        mixed = jnp.where(lane < heads, beta[at], total)
        place = step * (ROWS // CHUNK) + part
        cols_ref[place] = mixed
        turned_ref[place] = jnp.transpose(mixed)[: 2 * heads]


def chunk_maps(place, heads, keys_ref, values_ref, cols_ref, turned_ref, maps_ref):
    rows = pl.ds(pl.multiple_of(place * CHUNK, CHUNK), CHUNK)
    cols = cols_ref[place]
    i, j = iotas((CHUNK, CHUNK))
    left = j < HEAD
    apart = jnp.where(i > j, i ^ j, 0)
    one = jnp.where(i == j, 1.0, 0.0)
    zero = jnp.zeros((CHUNK, LANES), BF16)
    heads_of = []
    for h in range(heads):
        pair = slice(h // 2 * LANES, (h // 2 + 1) * LANES)
        keys = keys_ref[rows, pair]
        mine = left if h % 2 == 0 else ~left
        kh, kl = split(keys)
        mh, ml = split(jnp.where(mine, keys, 0.0))
        wide = jnp.concatenate([jnp.concatenate([kh, kh], axis=1), jnp.concatenate([kl, zero], axis=1)], axis=0)
        both = dot(jnp.concatenate([mh, ml], axis=1), wide, NT)
        gram = both[:, :CHUNK] + both[:, CHUNK:]
        beta = jnp.broadcast_to(cols[:, h : h + 1], (CHUNK, LANES))
        total = jnp.broadcast_to(cols[:, heads + h : heads + h + 1], (CHUNK, LANES))
        ahead = jnp.broadcast_to(turned_ref[place, heads + h : heads + h + 1, :], (CHUNK, LANES))
        lower = jnp.where(i > j, beta * gram * jnp.exp(total - ahead), 0.0)
        heads_of.append((lower, beta, total))
    inverses = [one - jnp.where(apart == 1, lower, 0.0) for lower, _, _ in heads_of]
    level = 1
    while 2 << level <= CHUNK:
        here = (apart >> level) == 1
        inner = [matmul(jnp.where(here, low[0], 0.0), inv) for low, inv in zip(heads_of, inverses)]
        inverses = [inv - matmul(inv, inn) for inv, inn in zip(inverses, inner)]
        level += 1
    for p in range(heads // 2):
        pair = slice(p * LANES, (p + 1) * LANES)
        keys = keys_ref[rows, pair]
        values = values_ref[rows, pair]
        turned = swapped(keys)
        carried, solved, closing = [], [], []
        for h in (2 * p, 2 * p + 1):
            mine = left if h % 2 == 0 else ~left
            _, beta, total = heads_of[h]
            right = beta * jnp.where(mine, values, -jnp.exp(total) * turned)
            solved.append(matmul(inverses[h], right))
            last = total[CHUNK - 1 :, :]
            carried.append(jnp.where(mine, keys * jnp.exp(last - total), 0.0))
            closing.append(jnp.exp(last))
        ch, cl = split(jnp.concatenate(carried, axis=0))
        sh, sl = split(jnp.concatenate(solved, axis=0))
        both = dot(ch, jnp.concatenate([sh, sl], axis=1), TN)
        tile = both[:, :LANES] + both[:, LANES:] + dot(cl, sh, TN)
        kept = jnp.where(i < HEAD, jnp.broadcast_to(closing[0], tile.shape), jnp.broadcast_to(closing[1], tile.shape))
        maps_ref[place, p] = tile + jnp.where(j == (i ^ HEAD), kept, 0.0)


def remote(src, dst, send, recv, to):
    return pltpu.make_async_remote_copy(
        src_ref=src, dst_ref=dst, send_sem=send, recv_sem=recv, device_id={"sp": to}, device_id_type=MESH
    )


def exchange(ring, near, tiles, near_ref, head_ref, far_ref, rows_ref, final_ref, probe_ref, sems):
    send1, recv1, send2, recv2, send3, recv3 = sems
    far = ring // near
    me = lax.axis_index("sp")
    place, block = lax.rem(me, near), lax.div(me, near)

    copies = []
    for k in range(1, near):
        to = lax.rem(place + k, near)
        copies.append(
            remote(tiles.at[to], near_ref.at[place], send1.at[k], recv1.at[k], block * near + to)
        )
        copies[-1].start()
    near_ref[place] = tiles[place]
    for copy in copies:
        copy.wait_recv()
    tile = near_ref[0]
    for k in range(1, near):
        tile = composed(near_ref[k], tile)

    head_ref[0] = tile[:HEAD]
    head_ref[1] = swapped(tile[HEAD:])
    side = lax.rem(block, 2)
    for k in range(1, far):
        to = lax.rem(block + k, far)
        copies.append(
            remote(head_ref.at[lax.rem(to, 2)], far_ref.at[block], send2.at[k], recv2.at[k], to * near + place)
        )
        copies[-1].start()
    far_ref[block] = head_ref[side]
    for copy in copies[near - 1 :]:
        copy.wait_recv()
    i, j = iotas((HEAD, LANES))
    below = jnp.zeros((HEAD, LANES), F32)
    state = far_ref[0]
    for k in range(1, far):
        later = far_ref[k]
        transfer = jnp.where(j < HEAD, swapped(later), 0.0)
        state = matmul(transfer, jnp.concatenate([state, below], axis=0)) + later

    slot = place * 2 + side
    probe = jnp.broadcast_to(probe_ref[pl.ds(slot, 1), :], (8, LANES))
    read = matmul(probe, jnp.concatenate([state, below], axis=0))
    rows = HEAD // ring
    for d in range(ring):
        rows_ref[d, :rows] = state[d * rows : (d + 1) * rows]
        rows_ref[d, rows : rows + 1] = read[:1]
    beside = lax.rem(block + 1 + (far - 2) * (1 - lax.div(place, near // 2)), far)
    targets = [block * near + lax.rem(place + k, near) for k in range(1, near)]
    targets += [beside * near + k for k in range(near)]
    last = []
    for k, to in enumerate(targets):
        last.append(remote(rows_ref.at[to], final_ref.at[slot], send3.at[k], recv3.at[slot], to))
        last[-1].start()
    final_ref[slot] = rows_ref[me]
    slots = 2 * near
    for k in range(1, slots):
        other = lax.rem(slot + k, slots)
        remote(rows_ref.at[0], final_ref.at[other], send3.at[0], recv3.at[other], me).wait_recv()
    for copy in copies + last:
        copy.wait_send()


def kernel(
    ring,
    heads,
    all_heads,
    x_hbm,
    wk_hbm,
    wv_hbm,
    wb_hbm,
    wf_hbm,
    speed_ref,
    extra_ref,
    probe_ref,
    states_ref,
    reads_ref,
    x_ref,
    w_ref,
    wb_ref,
    wf_ref,
    wg_ref,
    keys_ref,
    values_ref,
    cols_ref,
    turned_ref,
    maps_ref,
    tiles,
    near_ref,
    head_ref,
    far_ref,
    rows_ref,
    final_ref,
    q_ref,
    local_sems,
    x_sems,
    send1,
    recv1,
    send2,
    recv2,
    send3,
    recv3,
):
    me = lax.axis_index("sp")
    barrier = pltpu.get_barrier_semaphore()

    @pl.loop(1, ring)
    def _(k):
        pl.semaphore_signal(barrier, inc=1, device_id={"sp": lax.rem(me + k, ring)}, device_id_type=MESH)

    width = heads * HEAD
    seqs, span, _ = x_hbm.shape
    weights = [
        pltpu.make_async_copy(wb_hbm, wb_ref, local_sems.at[0]),
        pltpu.make_async_copy(wf_hbm, wf_ref, local_sems.at[1]),
        pltpu.make_async_copy(wk_hbm, w_ref.at[:, :width], local_sems.at[2]),
        pltpu.make_async_copy(wv_hbm, w_ref.at[:, width:], local_sems.at[3]),
    ]
    for copy in weights:
        copy.start()
    steps = seqs * span // ROWS
    for step in range(steps):
        s, first = divmod(step * ROWS, span)
        pltpu.make_async_copy(
            x_hbm.at[s, pl.ds(first, ROWS)], x_ref.at[pl.ds(step * ROWS, ROWS)], x_sems.at[step]
        ).start()

    for s in range(seqs):
        for h in range(heads):
            pair = probe_ref[s : s + 1, h // 2 * LANES : (h // 2 + 1) * LANES].astype(F32)
            pair = pair if h % 2 == 0 else swapped(pair)
            _, lane = iotas((1, LANES))
            q_ref[s * heads + h : s * heads + h + 1, :] = jnp.where(lane < HEAD, pair, 0.0)

    weights[0].wait()
    weights[1].wait()
    wg_ref[...] = jnp.concatenate(
        [wb_ref[...], wf_ref[...], jnp.zeros((wb_ref.shape[0], LANES - 2 * all_heads), BF16)], axis=1
    )
    weights[2].wait()
    weights[3].wait()

    @pl.loop(0, steps)
    def _(step):
        pltpu.make_async_copy(
            x_hbm.at[0, pl.ds(0, ROWS)], x_ref.at[pl.ds(step * ROWS, ROWS)], x_sems.at[step]
        ).wait()
        project(step, heads, all_heads, x_ref, w_ref, wg_ref, extra_ref, speed_ref, keys_ref, values_ref, cols_ref, turned_ref)

    chunks = span // CHUNK

    @pl.loop(0, seqs * chunks)
    def _(place):
        chunk_maps(place, heads, keys_ref, values_ref, cols_ref, turned_ref, maps_ref)

    for s in range(seqs):
        for p in range(heads // 2):
            parts = [maps_ref[s * chunks + n, p] for n in range(chunks)]
            while len(parts) > 1:
                parts = [composed(parts[n + 1], parts[n]) for n in range(0, len(parts), 2)]
            tiles[s * (heads // 2) + p] = parts[0]

    pl.semaphore_wait(barrier, ring - 1)
    near = seqs * heads // 2
    exchange(
        ring, near, tiles, near_ref, head_ref, far_ref, rows_ref, final_ref, q_ref,
        (send1, recv1, send2, recv2, send3, recv3),
    )

    rows = HEAD // ring
    _, lane = iotas((1, LANES))
    lines = []
    for s in range(seqs):
        line = []
        for h in range(heads):
            got = final_ref[s * heads + h]
            states_ref[s, h] = got[:rows, :HEAD].astype(BF16)
            read = jnp.where(lane < HEAD, got[rows : rows + 1], 0.0)
            read = read * lax.rsqrt(jnp.sum(read * read, axis=1, keepdims=True) / HEAD + 1e-06)
            line.append(read)
        pairs = [line[2 * p] + swapped(line[2 * p + 1]) for p in range(heads // 2)]
        lines.append(jnp.concatenate(pairs, axis=1))
    reads_ref[...] = jnp.concatenate(lines, axis=0).astype(BF16)


def body(
    ring,
    layer_feed,
    address_mapping,
    content_mapping,
    beta_mapping_matrix,
    forgetting_mapping,
    logged_fading_speed,
    extra_forgetting,
    opening_probe,
):
    seqs, span, depth = layer_feed.shape
    width = address_mapping.shape[1]
    heads = width // HEAD
    all_heads = beta_mapping_matrix.shape[1]
    tokens = seqs * span
    near = seqs * heads // 2
    places = tokens // CHUNK
    hbm = pl.BlockSpec(memory_space=pl.ANY)
    vmem = pl.BlockSpec(memory_space=pltpu.VMEM)
    dma = pltpu.SemaphoreType.DMA
    return pl.pallas_call(
        functools.partial(kernel, ring, heads, all_heads),
        out_shape=(
            jax.ShapeDtypeStruct((seqs, heads, HEAD // ring, HEAD), BF16),
            jax.ShapeDtypeStruct((seqs, width), BF16),
        ),
        in_specs=[hbm] * 5 + [pl.BlockSpec(memory_space=pltpu.SMEM), vmem, vmem],
        out_specs=(vmem, vmem),
        scratch_shapes=[
            pltpu.VMEM((tokens, depth), BF16),
            pltpu.VMEM((depth, 2 * width), BF16),
            pltpu.VMEM((depth, all_heads), BF16),
            pltpu.VMEM((depth, all_heads), BF16),
            pltpu.VMEM((depth, LANES), BF16),
            pltpu.VMEM((tokens, width), F32),
            pltpu.VMEM((tokens, width), F32),
            pltpu.VMEM((places, CHUNK, LANES), F32),
            pltpu.VMEM((places, 2 * heads, LANES), F32),
            pltpu.VMEM((places, heads // 2, LANES, LANES), F32),
            pltpu.VMEM((near, LANES, LANES), F32),
            pltpu.VMEM((near, LANES, LANES), F32),
            pltpu.VMEM((2, HEAD, LANES), F32),
            pltpu.VMEM((ring // near, HEAD, LANES), F32),
            pltpu.VMEM((ring, 8, LANES), F32),
            pltpu.VMEM((2 * near, 8, LANES), F32),
            pltpu.VMEM((seqs * heads, LANES), F32),
            dma((4,)),
            dma((tokens // ROWS,)),
            dma((near,)),
            dma((near,)),
            dma((ring // near,)),
            dma((ring // near,)),
            dma((2 * near - 1,)),
            dma((2 * near,)),
        ],
        compiler_params=pltpu.CompilerParams(
            collective_id=0, has_side_effects=True, vmem_limit_bytes=56 * 1024 * 1024
        ),
    )(
        layer_feed,
        address_mapping,
        content_mapping,
        beta_mapping_matrix,
        forgetting_mapping,
        logged_fading_speed,
        extra_forgetting.reshape(tokens, heads),
        opening_probe,
    )


def solution(mesh):
    in_specs = (
        P("grp", "sp", None),
        P(None, "tp"),
        P(None, "tp"),
        P(),
        P(),
        P("tp"),
        P("grp", "sp", "tp"),
        P("grp", "tp"),
    )
    out_specs = (P("grp", "tp", "sp", None), P("grp", "tp"))
    return jax.shard_map(
        functools.partial(body, mesh.shape["sp"]),
        mesh=mesh,
        in_specs=in_specs,
        out_specs=out_specs,
        check_vma=False,
    )
```

```python
import functools

import jax
import jax.numpy as jnp
from jax import lax
from jax.experimental import pallas as pl
from jax.experimental.pallas import tpu as pltpu
from jax.sharding import PartitionSpec as P

HEAD = 64
LANES = 128
CHUNK = 128
ROWS = 256
MESH = pl.DeviceIdType.MESH
F32 = jnp.float32
BF16 = jnp.bfloat16
NN = (((1,), (0,)), ((), ()))
NT = (((1,), (1,)), ((), ()))
TN = (((0,), (0,)), ((), ()))


def dot(left, right, dims=NN):
    return lax.dot_general(left, right, dims, preferred_element_type=F32)


def split(x):
    high = x.astype(BF16)
    return high, (x - high.astype(F32)).astype(BF16)


def matmul(left, right):
    lh, ll = split(left)
    rh, rl = split(right)
    wide = jnp.concatenate(
        [jnp.concatenate([rh, rl], axis=1), jnp.concatenate([rh, jnp.zeros_like(rh)], axis=1)], axis=0
    )
    both = dot(jnp.concatenate([lh, ll], axis=1), wide)
    return both[:, : right.shape[1]] + both[:, right.shape[1] :]


def iotas(shape):
    return lax.broadcasted_iota(jnp.int32, shape, 0), lax.broadcasted_iota(jnp.int32, shape, 1)


def swapped(x):
    return pltpu.roll(x, HEAD, 1)


def diagonal():
    i, j = iotas((LANES, LANES))
    return (i < HEAD) == (j < HEAD)


def composed(later, earlier):
    own = diagonal()
    return matmul(jnp.where(own, swapped(later), 0.0), earlier) + jnp.where(own, later, 0.0)


def silu(x):
    return x / (1.0 + jnp.exp(-x))


def halves(x):
    return jnp.concatenate(split(x), axis=1)


def stacked(left, right):
    count = left.shape[0]
    both = dot(jnp.concatenate(split(left), axis=0), right)
    both = both[:count] + both[count:]
    return both[:, :LANES] + both[:, LANES:]


def project(step, heads, x_ref, w_ref, gate_ref, extra_ref, speed_ref, keys_ref, values_ref, cols_ref, turned_ref):
    rows = pl.ds(pl.multiple_of(step * ROWS, ROWS), ROWS)
    x = x_ref[rows, :]
    width = heads * HEAD
    both = dot(x, w_ref[...]).astype(BF16).astype(F32)
    pre = dot(gate_ref[...], x, NT).astype(BF16).astype(F32)
    keys = silu(both[:, :width])
    high, low = split(keys * keys)
    i, j = iotas((width, width))
    same = jnp.where(i // HEAD == j // HEAD, 1.0, 0.0).astype(BF16)
    squares = dot(high, same) + dot(low, same)
    keys_ref[rows, :] = keys * lax.rsqrt(squares + 1e-06)
    values_ref[rows, :] = silu(both[:, width:])

    spans = extra_ref.shape[2] // ROWS
    at = pl.ds(pl.multiple_of(lax.rem(step, spans) * ROWS, ROWS), ROWS)
    extra = extra_ref[lax.div(step, spans), :, at].astype(F32)
    extra = jnp.concatenate([extra, jnp.zeros((8 - heads, ROWS), F32)], axis=0)
    i, _ = iotas((8, ROWS))
    speed = jnp.zeros((8, ROWS), F32)
    for h in range(heads):
        speed = jnp.where(i == h, speed_ref[h], speed)
    beta = 1.0 / (1.0 + jnp.exp(-pre[:8]))
    fade = pre[8:]
    plus = jnp.maximum(fade, 0.0) + jnp.log(1.0 + jnp.exp(-jnp.abs(fade)))
    decay = -jnp.exp(speed) * plus + extra
    i, j = iotas((CHUNK, CHUNK))
    until = jnp.where(i <= j, 1.0, 0.0)
    for part in range(ROWS // CHUNK):
        at = slice(part * CHUNK, (part + 1) * CHUNK)
        total = lax.dot_general(
            decay[:, at], until, NN, precision=lax.Precision.HIGHEST, preferred_element_type=F32
        )
        mixed = jnp.concatenate([beta[:, at], total], axis=0)
        place = step * (ROWS // CHUNK) + part
        turned_ref[place] = mixed
        cols_ref[place] = jnp.transpose(mixed)


def lower_part(place, h, keys_ref, cols_ref, turned_ref):
    rows = pl.ds(pl.multiple_of(place * CHUNK, CHUNK), CHUNK)
    i, j = iotas((CHUNK, CHUNK))
    keys = keys_ref[rows, h // 2 * LANES : (h // 2 + 1) * LANES]
    mine = (j < HEAD) if h % 2 == 0 else (j >= HEAD)
    kh, kl = split(keys)
    mh, ml = split(jnp.where(mine, keys, 0.0))
    wide = jnp.concatenate([jnp.concatenate([kh, kh], axis=1), jnp.concatenate([kl, jnp.zeros_like(kl)], axis=1)], axis=0)
    both = dot(jnp.concatenate([mh, ml], axis=1), wide, NT)
    gram = both[:, :CHUNK] + both[:, CHUNK:]
    beta = jnp.broadcast_to(cols_ref[place, :, h : h + 1], (CHUNK, LANES))
    total = jnp.broadcast_to(cols_ref[place, :, 8 + h : 9 + h], (CHUNK, LANES))
    ahead = jnp.broadcast_to(turned_ref[place, 8 + h : 9 + h, :], (CHUNK, LANES))
    return jnp.where(i > j, beta * gram * jnp.exp(total - ahead), 0.0)


def chunk_map(place, p, inverses, keys_ref, values_ref, cols_ref):
    rows = pl.ds(pl.multiple_of(place * CHUNK, CHUNK), CHUNK)
    pair = slice(p * LANES, (p + 1) * LANES)
    i, j = iotas((CHUNK, CHUNK))
    keys = keys_ref[rows, pair]
    values = values_ref[rows, pair]
    turned = swapped(keys)
    carried, solved, closing = [], [], []
    for h, inverse in zip((2 * p, 2 * p + 1), inverses):
        mine = (j < HEAD) if h % 2 == 0 else (j >= HEAD)
        beta = jnp.broadcast_to(cols_ref[place, :, h : h + 1], (CHUNK, LANES))
        total = jnp.broadcast_to(cols_ref[place, :, 8 + h : 9 + h], (CHUNK, LANES))
        solved.append(matmul(inverse, beta * jnp.where(mine, values, -jnp.exp(total) * turned)))
        last = total[CHUNK - 1 :, :]
        carried.append(jnp.where(mine, keys * jnp.exp(last - total), 0.0))
        closing.append(jnp.exp(last))
    ch, cl = split(jnp.concatenate(carried, axis=0))
    sh, sl = split(jnp.concatenate(solved, axis=0))
    both = dot(ch, jnp.concatenate([sh, sl], axis=1), TN)
    tile = both[:, :LANES] + both[:, LANES:] + dot(cl, sh, TN)
    kept = jnp.where(i < HEAD, jnp.broadcast_to(closing[0], tile.shape), jnp.broadcast_to(closing[1], tile.shape))
    return tile + jnp.where(j == (i ^ HEAD), kept, 0.0)


SMALL = 16


def sequence_maps(s, chunks, heads, keys_ref, values_ref, cols_ref, turned_ref, low_ref, near_low_ref, tiles):
    places = [s * chunks + n for n in range(chunks)]
    chains = [(n, h) for n in range(chunks) for h in range(heads)]
    count = CHUNK // SMALL
    i, j = iotas((CHUNK, CHUNK))
    same = (i // SMALL) == (j // SMALL)
    same_bf = jnp.where(same, 1.0, 0.0).astype(BF16)
    apart = jnp.where(i > j, i ^ j, 0)
    r, l = iotas((SMALL, LANES))
    c = l % SMALL
    close = jnp.where(r > c, r ^ c, 0)
    unit = jnp.where(r == c, 1.0, 0.0)

    state = []
    for slot, (n, h) in enumerate(chains):
        lower = lower_part(places[n], h, keys_ref, cols_ref, turned_ref)
        low_ref[slot] = halves(lower)
        inside = jnp.where(same, lower, 0.0)
        near_low_ref[slot] = halves(inside)
        packed = inside[:SMALL]
        for b in range(1, count):
            packed = packed + inside[b * SMALL : (b + 1) * SMALL]
        state.append(unit - jnp.where(close == 1, packed, 0.0))
    level = 1
    while 2 << level <= SMALL:
        inner = [stacked(x, near_low_ref[slot]) for slot, x in enumerate(state)]
        spread = []
        for x in state:
            high, low = split(x)
            high = jnp.concatenate([high] * count, axis=0) * same_bf
            low = jnp.concatenate([low] * count, axis=0) * same_bf
            spread.append(jnp.concatenate([high, low], axis=1))
        inner = [stacked(y, wide) for y, wide in zip(inner, spread)]
        state = [x - jnp.where((close >> level) == 1, y, 0.0) for x, y in zip(state, inner)]
        level += 1
    state = [jnp.where(same, jnp.concatenate([x] * count, axis=0), 0.0) for x in state]
    while 2 << level <= CHUNK:
        size = 1 << level
        odd = [slice(b * size, (b + 1) * size) for b in range(1, CHUNK // size, 2)]
        even = [slice(b * size, (b + 1) * size) for b in range(0, CHUNK // size, 2)]
        here = jnp.concatenate([apart[at] for at in odd], axis=0)
        part = [jnp.concatenate([x[at] for at in odd], axis=0) for x in state]
        inner = [stacked(x, low_ref[slot]) for slot, x in enumerate(part)]
        inner = [stacked(y, halves(x)) for y, x in zip(inner, state)]
        part = [x - jnp.where((here >> level) == 1, y, 0.0) for x, y in zip(part, inner)]
        state = [
            jnp.concatenate(
                [z for b, at in enumerate(even) for z in (x[at], y[b * size : (b + 1) * size])], axis=0
            )
            for x, y in zip(state, part)
        ]
        level += 1
    for p in range(heads // 2):
        parts = [
            chunk_map(places[n], p, state[n * heads + 2 * p : n * heads + 2 * p + 2], keys_ref, values_ref, cols_ref)
            for n in range(chunks)
        ]
        while len(parts) > 1:
            parts = [composed(parts[n + 1], parts[n]) for n in range(0, len(parts), 2)]
        tiles[s * (heads // 2) + p] = parts[0]


def remote(src, dst, send, recv, to):
    return pltpu.make_async_remote_copy(
        src_ref=src, dst_ref=dst, send_sem=send, recv_sem=recv, device_id={"sp": to}, device_id_type=MESH
    )


def greet(ring, near, me, barrier):
    far = ring // near
    place, block = lax.rem(me, near), lax.div(me, near)

    def tell(to):
        pl.semaphore_signal(barrier, inc=1, device_id={"sp": to}, device_id_type=MESH)

    for k in range(1, near):
        tell(block * near + lax.rem(place + k, near))

    @pl.when(block > 0)
    def _():
        tell(me - near)

    @pl.when(block < far - 1)
    def _():
        for k in range(near):
            tell((far - 1) * near + k)


def exchange(ring, near, me, tiles, near_ref, state_ref, prior_ref, rows_ref, final_ref, probe_ref, sems):
    recv1, send2, recv2, send3, recv3 = sems
    far = ring // near
    place, block = lax.rem(me, near), lax.div(me, near)
    own = diagonal()

    near_ref[place] = tiles[place]

    def arrived(k):
        @pl.when(place != k)
        def _():
            remote(tiles.at[0], near_ref.at[k], send2, recv1.at[k], me).wait_recv()

    arrived(0)
    tile = near_ref[0]
    for k in range(1, near - 1):
        arrived(k)
        tile = composed(near_ref[k], tile)

    carry = remote(state_ref, prior_ref, send2, recv2, lax.rem(me + near, ring))

    @pl.when(block == 0)
    def _():
        prior_ref[...] = jnp.zeros_like(prior_ref)

    @pl.when(block > 0)
    def _():
        carry.wait_recv()

    prior = prior_ref[...]
    state = composed(tile, jnp.where(own, jnp.concatenate([prior, prior], axis=0), 0.0))
    arrived(near - 1)
    state = composed(near_ref[near - 1], state)
    state = jnp.where(own, state, 0.0)
    both = state[:HEAD] + state[HEAD:]

    @pl.when(block < far - 1)
    def _():
        state_ref[...] = both
        carry.start()

    @pl.when(block == far - 1)
    def _():
        rows = HEAD // ring
        read = matmul(jnp.broadcast_to(probe_ref[pl.ds(place, 1), :], (8, LANES)), state)
        for d in range(ring):
            rows_ref[d, :rows] = both[d * rows : (d + 1) * rows]
            rows_ref[d, rows : rows + 1] = read[:1]

        @pl.loop(1, ring)
        def _(k):
            to = lax.rem(me + k, ring)
            remote(rows_ref.at[to], final_ref.at[place], send3.at[k], recv3.at[place], to).start()

        final_ref[place] = rows_ref[me]

    for k in range(near):
        @pl.when((block < far - 1) | (place != k))
        def _():
            remote(rows_ref.at[0], final_ref.at[k], send3.at[0], recv3.at[k], me).wait_recv()

    @pl.when(block < far - 1)
    def _():
        carry.wait_send()

    @pl.when(block == far - 1)
    def _():
        @pl.loop(1, ring)
        def _(k):
            remote(rows_ref.at[0], final_ref.at[place], send3.at[k], recv3.at[place], me).wait_send()


def kernel(
    ring,
    heads,
    all_heads,
    x_hbm,
    wk_hbm,
    wv_hbm,
    wb_hbm,
    wf_hbm,
    speed_ref,
    extra_ref,
    probe_ref,
    states_ref,
    reads_ref,
    x_ref,
    w_ref,
    wg_ref,
    gate_ref,
    keys_ref,
    values_ref,
    cols_ref,
    turned_ref,
    low_ref,
    near_low_ref,
    tiles,
    near_ref,
    state_ref,
    prior_ref,
    rows_ref,
    final_ref,
    q_ref,
    local_sems,
    x_sems,
    send1,
    recv1,
    send2,
    recv2,
    send3,
    recv3,
):
    me = lax.axis_index("sp")
    width = heads * HEAD
    seqs, span, _ = x_hbm.shape
    pairs = heads // 2
    near = seqs * pairs
    far = ring // near
    barrier = pltpu.get_barrier_semaphore()
    weights = [
        pltpu.make_async_copy(wb_hbm, wg_ref.at[:all_heads], local_sems.at[0]),
        pltpu.make_async_copy(wf_hbm, wg_ref.at[all_heads:], local_sems.at[1]),
        pltpu.make_async_copy(wk_hbm, w_ref.at[:, :width], local_sems.at[2]),
        pltpu.make_async_copy(wv_hbm, w_ref.at[:, width:], local_sems.at[3]),
    ]
    for copy in weights:
        copy.start()
    steps = span // ROWS
    for step in range(seqs * steps):
        s, first = divmod(step * ROWS, span)
        pltpu.make_async_copy(
            x_hbm.at[s, pl.ds(first, ROWS)], x_ref.at[pl.ds(step * ROWS, ROWS)], x_sems.at[step]
        ).start()
    greet(ring, near, me, barrier)
    for s in range(seqs):
        for p in range(pairs):
            q_ref[s * pairs + p : s * pairs + p + 1, :] = probe_ref[s : s + 1, p * LANES : (p + 1) * LANES].astype(F32)

    weights[0].wait()
    weights[1].wait()
    first = lax.axis_index("tp") * heads
    i, j = iotas((16, 2 * all_heads))
    taken = ((i < heads) & (j == first + i)) | ((i >= 8) & (i < 8 + heads) & (j == all_heads + first + i - 8))
    gate_ref[...] = dot(jnp.where(taken, 1.0, 0.0).astype(BF16), wg_ref[...]).astype(BF16)
    weights[2].wait()
    weights[3].wait()

    place, block = lax.rem(me, near), lax.div(me, near)

    def near_copy(pair):
        return remote(tiles.at[pair], near_ref.at[place], send1.at[pair], recv1.at[place], block * near + pair)

    @pl.loop(0, seqs)
    def _(s):
        @pl.loop(0, steps)
        def _(part):
            step = s * steps + part
            pltpu.make_async_copy(
                x_hbm.at[0, pl.ds(0, ROWS)], x_ref.at[pl.ds(step * ROWS, ROWS)], x_sems.at[step]
            ).wait()
            project(step, heads, x_ref, w_ref, gate_ref, extra_ref, speed_ref, keys_ref, values_ref, cols_ref, turned_ref)

        sequence_maps(
            s, span // CHUNK, heads, keys_ref, values_ref, cols_ref, turned_ref, low_ref, near_low_ref, tiles
        )

        @pl.when(s == 0)
        def _():
            pl.semaphore_wait(barrier, jnp.where(block == far - 1, ring - 1, near))

        for p in range(pairs):
            @pl.when(place != s * pairs + p)
            def _():
                near_copy(s * pairs + p).start()

    exchange(
        ring, near, me, tiles, near_ref, state_ref, prior_ref, rows_ref, final_ref, q_ref,
        (recv1, send2, recv2, send3, recv3),
    )
    for pair in range(near):
        @pl.when(place != pair)
        def _():
            near_copy(pair).wait_send()

    rows = HEAD // ring
    _, lane = iotas((1, LANES))
    for s in range(seqs):
        for p in range(pairs):
            got = final_ref[s * pairs + p]
            states_ref[s, 2 * p] = got[:rows, :HEAD].astype(BF16)
            states_ref[s, 2 * p + 1] = swapped(got)[:rows, :HEAD].astype(BF16)
            read = got[rows : rows + 1]
            square = read * read
            even = jnp.sum(jnp.where(lane < HEAD, square, 0.0), axis=1, keepdims=True)
            odd = jnp.sum(jnp.where(lane < HEAD, 0.0, square), axis=1, keepdims=True)
            mean = jnp.where(lane < HEAD, even, odd) / HEAD
            reads_ref[s : s + 1, p * LANES : (p + 1) * LANES] = (read * lax.rsqrt(mean + 1e-06)).astype(BF16)


def body(
    ring,
    layer_feed,
    address_mapping,
    content_mapping,
    beta_mapping_matrix,
    forgetting_mapping,
    logged_fading_speed,
    extra_forgetting,
    opening_probe,
):
    seqs, span, depth = layer_feed.shape
    width = address_mapping.shape[1]
    heads = width // HEAD
    all_heads = beta_mapping_matrix.shape[1]
    tokens = seqs * span
    near = seqs * heads // 2
    places = tokens // CHUNK
    chains = span // CHUNK * heads
    hbm = pl.BlockSpec(memory_space=pl.ANY)
    vmem = pl.BlockSpec(memory_space=pltpu.VMEM)
    dma = pltpu.SemaphoreType.DMA
    return pl.pallas_call(
        functools.partial(kernel, ring, heads, all_heads),
        out_shape=(
            jax.ShapeDtypeStruct((seqs, heads, HEAD // ring, HEAD), BF16),
            jax.ShapeDtypeStruct((seqs, width), BF16),
        ),
        in_specs=[hbm] * 5 + [pl.BlockSpec(memory_space=pltpu.SMEM), vmem, vmem],
        out_specs=(vmem, vmem),
        scratch_shapes=[
            pltpu.VMEM((tokens, depth), BF16),
            pltpu.VMEM((depth, 2 * width), BF16),
            pltpu.VMEM((2 * all_heads, depth), BF16),
            pltpu.VMEM((16, depth), BF16),
            pltpu.VMEM((tokens, width), F32),
            pltpu.VMEM((tokens, width), F32),
            pltpu.VMEM((places, CHUNK, 16), F32),
            pltpu.VMEM((places, 16, LANES), F32),
            pltpu.VMEM((chains, CHUNK, 2 * CHUNK), BF16),
            pltpu.VMEM((chains, CHUNK, 2 * CHUNK), BF16),
            pltpu.VMEM((near, LANES, LANES), F32),
            pltpu.VMEM((near, LANES, LANES), F32),
            pltpu.VMEM((HEAD, LANES), F32),
            pltpu.VMEM((HEAD, LANES), F32),
            pltpu.VMEM((ring, 8, LANES), F32),
            pltpu.VMEM((near, 8, LANES), F32),
            pltpu.VMEM((near, LANES), F32),
            dma((4,)),
            dma((tokens // ROWS,)),
            dma((near,)),
            dma((near,)),
            dma,
            dma,
            dma((ring,)),
            dma((near,)),
        ],
        compiler_params=pltpu.CompilerParams(
            collective_id=0, has_side_effects=True, vmem_limit_bytes=56 * 1024 * 1024
        ),
    )(
        layer_feed,
        address_mapping,
        content_mapping,
        beta_mapping_matrix.T,
        forgetting_mapping.T,
        logged_fading_speed,
        extra_forgetting.transpose(0, 2, 1),
        opening_probe,
    )


def solution(mesh):
    in_specs = (
        P("grp", "sp", None),
        P(None, "tp"),
        P(None, "tp"),
        P(),
        P(),
        P("tp"),
        P("grp", "sp", "tp"),
        P("grp", "tp"),
    )
    out_specs = (P("grp", "tp", "sp", None), P("grp", "tp"))
    return jax.shard_map(
        functools.partial(body, mesh.shape["sp"]),
        mesh=mesh,
        in_specs=in_specs,
        out_specs=out_specs,
        check_vma=False,
    )
```

```python
import functools

import jax
import jax.numpy as jnp
from jax import lax
from jax.experimental import pallas as pl
from jax.experimental.pallas import tpu as pltpu
from jax.sharding import PartitionSpec as P

HEAD = 64
LANES = 128
CHUNK = 128
ROWS = 256
PIECES = 4
MESH = pl.DeviceIdType.MESH
F32 = jnp.float32
BF16 = jnp.bfloat16
NN = (((1,), (0,)), ((), ()))
NT = (((1,), (1,)), ((), ()))
TN = (((0,), (0,)), ((), ()))


def dot(left, right, dims=NN):
    return lax.dot_general(left, right, dims, preferred_element_type=F32)


def split(x):
    high = x.astype(BF16)
    return high, (x - high.astype(F32)).astype(BF16)


def matmul(left, right):
    lh, ll = split(left)
    rh, rl = split(right)
    wide = jnp.concatenate(
        [jnp.concatenate([rh, rl], axis=1), jnp.concatenate([rh, jnp.zeros_like(rh)], axis=1)], axis=0
    )
    both = dot(jnp.concatenate([lh, ll], axis=1), wide)
    return both[:, : right.shape[1]] + both[:, right.shape[1] :]


def iotas(shape):
    return lax.broadcasted_iota(jnp.int32, shape, 0), lax.broadcasted_iota(jnp.int32, shape, 1)


def swapped(x):
    return pltpu.roll(x, HEAD, 1)


def diagonal():
    i, j = iotas((LANES, LANES))
    return (i < HEAD) == (j < HEAD)


def composed(later, earlier):
    own = diagonal()
    return matmul(jnp.where(own, swapped(later), 0.0), earlier) + jnp.where(own, later, 0.0)


def silu(x):
    return x / (1.0 + jnp.exp(-x))


def project(
    step, heads, pieces, x_ref, w_ref, gate_ref, extra_ref, speed_ref, keys_ref, values_ref, cols_ref, turned_ref
):
    rows = pl.ds(pl.multiple_of(step * ROWS, ROWS), ROWS)
    width = heads * HEAD
    depth = x_ref.shape[1] // len(pieces)
    both = pre = None
    for k, arrive in enumerate(pieces):
        arrive()
        at = slice(k * depth, (k + 1) * depth)
        x = x_ref[rows, at]
        part, gates = dot(x, w_ref[at, :]), dot(gate_ref[:, at], x, NT)
        both, pre = (part, gates) if k == 0 else (both + part, pre + gates)
    both = both.astype(BF16).astype(F32)
    pre = pre.astype(BF16).astype(F32)
    keys = silu(both[:, :width])
    i, j = iotas((width, width))
    same = jnp.where(i // HEAD == j // HEAD, 1.0, 0.0).astype(BF16)
    squares = dot((keys * keys).astype(BF16), same)
    keys_ref[rows, :] = (keys * lax.rsqrt(squares + 1e-06)).astype(BF16)
    values_ref[rows, :] = silu(both[:, width:]).astype(BF16)

    spans = extra_ref.shape[2] // ROWS
    at = pl.ds(pl.multiple_of(lax.rem(step, spans) * ROWS, ROWS), ROWS)
    extra = extra_ref[lax.div(step, spans), :, at].astype(F32)
    extra = jnp.concatenate([extra, jnp.zeros((8 - heads, ROWS), F32)], axis=0)
    i, _ = iotas((8, ROWS))
    speed = jnp.zeros((8, ROWS), F32)
    for h in range(heads):
        speed = jnp.where(i == h, speed_ref[h], speed)
    beta = 1.0 / (1.0 + jnp.exp(-pre[:8]))
    fade = pre[8:]
    plus = jnp.maximum(fade, 0.0) + jnp.log(1.0 + jnp.exp(-jnp.abs(fade)))
    decay = -jnp.exp(speed) * plus + extra
    i, j = iotas((CHUNK, CHUNK))
    until = jnp.where(i <= j, 1.0, 0.0)
    for part in range(ROWS // CHUNK):
        at = slice(part * CHUNK, (part + 1) * CHUNK)
        total = lax.dot_general(
            decay[:, at], until, NN, precision=lax.Precision.HIGHEST, preferred_element_type=F32
        )
        mixed = jnp.concatenate([beta[:, at], total], axis=0)
        place = step * (ROWS // CHUNK) + part
        turned_ref[place] = mixed
        cols_ref[place] = jnp.transpose(mixed)


def lower_parts(place, p, keys_ref, cols_ref, turned_ref):
    rows = pl.ds(pl.multiple_of(place * CHUNK, CHUNK), CHUNK)
    i, j = iotas((CHUNK, CHUNK))
    left = jnp.where(j < HEAD, 1.0, 0.0).astype(BF16)
    keys = keys_ref[rows, p * LANES : (p + 1) * LANES]
    even = keys * left
    gram = dot(jnp.concatenate([even, keys - even], axis=0), keys, NT)
    parts = []
    for side in range(2):
        h = 2 * p + side
        beta = jnp.broadcast_to(cols_ref[place, :, h : h + 1], (CHUNK, LANES))
        total = jnp.broadcast_to(cols_ref[place, :, 8 + h : 9 + h], (CHUNK, LANES))
        ahead = jnp.broadcast_to(turned_ref[place, 8 + h : 9 + h, :], (CHUNK, LANES))
        lower = beta * gram[side * CHUNK : (side + 1) * CHUNK] * jnp.exp(total - ahead)
        parts.append(jnp.where(i > j, lower, 0.0).astype(BF16))
    return parts


def chunk_map(place, p, inverses, keys_ref, values_ref, cols_ref):
    rows = pl.ds(pl.multiple_of(place * CHUNK, CHUNK), CHUNK)
    pair = slice(p * LANES, (p + 1) * LANES)
    i, j = iotas((CHUNK, CHUNK))
    keys = keys_ref[rows, pair].astype(F32)
    values = values_ref[rows, pair].astype(F32)
    turned = swapped(keys)
    carried, solved, closing = [], [], []
    for h, inverse in zip((2 * p, 2 * p + 1), inverses):
        mine = (j < HEAD) if h % 2 == 0 else (j >= HEAD)
        beta = jnp.broadcast_to(cols_ref[place, :, h : h + 1], (CHUNK, LANES))
        total = jnp.broadcast_to(cols_ref[place, :, 8 + h : 9 + h], (CHUNK, LANES))
        right = beta * jnp.where(mine, values, -jnp.exp(total) * turned)
        solved.append(dot(inverse, right.astype(BF16)).astype(BF16))
        last = total[CHUNK - 1 :, :]
        carried.append(jnp.where(mine, keys * jnp.exp(last - total), 0.0).astype(BF16))
        closing.append(jnp.exp(last))
    tile = dot(jnp.concatenate(carried, axis=0), jnp.concatenate(solved, axis=0), TN)
    kept = jnp.where(i < HEAD, jnp.broadcast_to(closing[0], tile.shape), jnp.broadcast_to(closing[1], tile.shape))
    return tile + jnp.where(j == (i ^ HEAD), kept, 0.0)


SMALL = 16


def sequence_maps(s, chunks, heads, keys_ref, values_ref, cols_ref, turned_ref, low_ref, tiles):
    places = [s * chunks + n for n in range(chunks)]
    count = CHUNK // SMALL
    i, j = iotas((CHUNK, CHUNK))
    same = jnp.where((i // SMALL) == (j // SMALL), 1.0, 0.0).astype(BF16)
    apart = jnp.where(i > j, i ^ j, 0)
    r, l = iotas((SMALL, LANES))
    c = l % SMALL
    close = jnp.where(r > c, r ^ c, 0)
    unit = jnp.where(r == c, 1.0, 0.0)

    state = []
    for n in range(chunks):
        for p in range(heads // 2):
            for lower in lower_parts(places[n], p, keys_ref, cols_ref, turned_ref):
                low_ref[len(state)] = lower
                inside = lower * same
                packed = inside[:SMALL]
                for b in range(1, count):
                    packed = packed + inside[b * SMALL : (b + 1) * SMALL]
                state.append((unit - jnp.where(close == 1, packed.astype(F32), 0.0)).astype(BF16))
    level = 1
    while 2 << level <= SMALL:
        inner = [dot(x, low_ref[slot] * same).astype(BF16) for slot, x in enumerate(state)]
        inner = [dot(y, jnp.concatenate([x] * count, axis=0) * same) for x, y in zip(state, inner)]
        state = [x - jnp.where((close >> level) == 1, y, 0.0).astype(BF16) for x, y in zip(state, inner)]
        level += 1
    state = [jnp.concatenate([x] * count, axis=0) * same for x in state]
    while 2 << level <= CHUNK:
        size = 1 << level
        odd = [slice(b * size, (b + 1) * size) for b in range(1, CHUNK // size, 2)]
        even = [slice(b * size, (b + 1) * size) for b in range(0, CHUNK // size, 2)]
        here = jnp.concatenate([apart[at] for at in odd], axis=0)
        part = [jnp.concatenate([x[at] for at in odd], axis=0) for x in state]
        inner = [dot(x, low_ref[slot]).astype(BF16) for slot, x in enumerate(part)]
        inner = [dot(y, x) for y, x in zip(inner, state)]
        part = [x - jnp.where((here >> level) == 1, y, 0.0).astype(BF16) for x, y in zip(part, inner)]
        state = [
            jnp.concatenate(
                [z for b, at in enumerate(even) for z in (x[at], y[b * size : (b + 1) * size])], axis=0
            )
            for x, y in zip(state, part)
        ]
        level += 1
    for p in range(heads // 2):
        parts = [
            chunk_map(places[n], p, state[n * heads + 2 * p : n * heads + 2 * p + 2], keys_ref, values_ref, cols_ref)
            for n in range(chunks)
        ]
        while len(parts) > 1:
            parts = [composed(parts[n + 1], parts[n]) for n in range(0, len(parts), 2)]
        tiles[s * (heads // 2) + p] = parts[0]


def remote(src, dst, send, recv, to):
    return pltpu.make_async_remote_copy(
        src_ref=src, dst_ref=dst, send_sem=send, recv_sem=recv, device_id={"sp": to}, device_id_type=MESH
    )


def signal(semaphore, to):
    pl.semaphore_signal(semaphore, inc=1, device_id={"sp": to}, device_id_type=MESH)


def greet(ring, near, me, barrier):
    far = ring // near
    place, block = lax.rem(me, near), lax.div(me, near)
    for k in range(1, near):
        signal(barrier, block * near + lax.rem(place + k, near))

    @pl.when(block < far - 1)
    def _():
        for k in range(near):
            signal(barrier, (far - 1) * near + k)


def met(ring, near, me, barrier, ready):
    far = ring // near
    place, block = lax.rem(me, near), lax.div(me, near)
    pl.semaphore_wait(barrier, jnp.where(block == far - 1, ring - 1, near - 1))

    @pl.when((block == far - 1) & (place > 0))
    def _():
        signal(ready, 0)
        for b in range(far - 1):
            signal(ready, b * near + place)


def owner(pair):
    return jnp.maximum(pair, 1), jnp.where(pair == 0, 1, 0)


def exchange(ring, near, me, tiles, near_ref, sent_ref, far_ref, first_ref, rows_ref, final_ref, probe_ref, sems):
    recv1, send2, recv2, send_first, recv_first, send3, recv3, ready = sems
    far = ring // near
    place, block = lax.rem(me, near), lax.div(me, near)
    own = diagonal()
    i, j = iotas((LANES, LANES))

    firsts = []
    for pair in range(near):
        to, slot = max(pair, 1), int(pair == 0)
        firsts.append(
            remote(
                sent_ref.at[pair, :HEAD], first_ref.at[slot], send_first.at[pair], recv_first.at[slot],
                (far - 1) * near + to,
            )
        )

    @pl.when(me == 0)
    def _():
        for pair in range(near):
            tile = jnp.where(own, tiles[pair], 0.0)
            sent_ref[pair, :HEAD] = tile[:HEAD] + tile[HEAD:]
        pl.semaphore_wait(ready, near - 1)
        for copy in firsts:
            copy.start()

    outs = [
        remote(
            sent_ref.at[slot], far_ref.at[slot, jnp.minimum(block, far - 2)], send2.at[slot],
            recv2.at[slot, jnp.minimum(block, far - 2)], (far - 1) * near + place,
        )
        for slot in range(2)
    ]

    def final_copy(slot, pair, k):
        to = lax.rem(me + k, ring)
        return remote(rows_ref.at[slot, to], final_ref.at[pair], send3.at[slot, k], recv3.at[pair], to)

    @pl.when((block < far - 1) & (place > 0))
    def _():
        pl.semaphore_wait(ready, 1)

    for slot in (1, 0):
        pair = 0 if slot else place

        @pl.when((place == 1) if slot else (place > 0))
        def _():
            near_ref[slot, place] = tiles[pair]

            @pl.when(block == 0)
            def _():
                near_ref[slot, 0] = jnp.where(j == (i ^ HEAD), 1.0, 0.0)

            def arrived(k):
                @pl.when((place != k) & ((block > 0) | (k > 0)))
                def _():
                    remote(tiles.at[0], near_ref.at[slot, k], send2.at[0], recv1.at[slot, k], me).wait_recv()

            arrived(0)
            tile = near_ref[slot, 0]
            for k in range(1, near):
                arrived(k)
                tile = composed(near_ref[slot, k], tile)

            @pl.when(block < far - 1)
            def _():
                sent_ref[slot] = tile
                outs[slot].start()

            @pl.when(block == far - 1)
            def _():
                remote(sent_ref.at[0, :HEAD], first_ref.at[slot], send2.at[0], recv_first.at[slot], me).wait_recv()
                state = first_ref[slot]
                state = jnp.where(own, jnp.concatenate([state, state], axis=0), 0.0)
                for b in range(far - 1):
                    remote(sent_ref.at[0], far_ref.at[slot, b], send2.at[0], recv2.at[slot, b], me).wait_recv()
                    state = composed(far_ref[slot, b], state)
                state = jnp.where(own, composed(tile, state), 0.0)
                both = state[:HEAD] + state[HEAD:]
                rows = HEAD // ring
                read = matmul(jnp.broadcast_to(probe_ref[pl.ds(pair, 1), :], (8, LANES)), state)
                for d in range(ring):
                    rows_ref[slot, d, :rows] = both[d * rows : (d + 1) * rows]
                    rows_ref[slot, d, rows : rows + 1] = read[:1]

                @pl.loop(1, ring)
                def _(k):
                    final_copy(slot, pair, k).start()

                final_ref[pair] = rows_ref[slot, me]

    for pair in range(near):
        @pl.when((block < far - 1) | (place != max(pair, 1)))
        def _():
            remote(rows_ref.at[0, 0], final_ref.at[pair], send3.at[0, 0], recv3.at[pair], me).wait_recv()

    @pl.when(me == 0)
    def _():
        for copy in firsts:
            copy.wait_send()

    for slot in (1, 0):
        active = (place == 1) if slot else (place > 0)

        @pl.when(active & (block < far - 1))
        def _():
            outs[slot].wait_send()

        @pl.when(active & (block == far - 1))
        def _():
            @pl.loop(1, ring)
            def _(k):
                final_copy(slot, 0 if slot else place, k).wait_send()


def kernel(
    ring,
    heads,
    all_heads,
    x_hbm,
    wk_hbm,
    wv_hbm,
    wb_hbm,
    wf_hbm,
    speed_ref,
    extra_ref,
    probe_ref,
    states_ref,
    reads_ref,
    x_ref,
    w_ref,
    wg_ref,
    gate_ref,
    keys_ref,
    values_ref,
    cols_ref,
    turned_ref,
    low_ref,
    tiles,
    near_ref,
    sent_ref,
    far_ref,
    first_ref,
    rows_ref,
    final_ref,
    q_ref,
    gate_sems,
    w_sems,
    x_sems,
    send1,
    recv1,
    send2,
    recv2,
    send_first,
    recv_first,
    send3,
    recv3,
    ready,
):
    me = lax.axis_index("sp")
    width = heads * HEAD
    seqs, span, _ = x_hbm.shape
    pairs = heads // 2
    near = seqs * pairs
    far = ring // near
    barrier = pltpu.get_barrier_semaphore()
    gates = [
        pltpu.make_async_copy(wb_hbm, wg_ref.at[:all_heads], gate_sems.at[0]),
        pltpu.make_async_copy(wf_hbm, wg_ref.at[all_heads:], gate_sems.at[1]),
    ]
    for copy in gates:
        copy.start()
    depth = x_hbm.shape[2] // PIECES
    steps = span // ROWS
    first_pieces = []
    for k in range(PIECES):
        at = pl.ds(k * depth, depth)
        first_pieces.append([
            pltpu.make_async_copy(wk_hbm.at[at], w_ref.at[at, :width], w_sems.at[0, k]),
            pltpu.make_async_copy(wv_hbm.at[at], w_ref.at[at, width:], w_sems.at[1, k]),
            pltpu.make_async_copy(x_hbm.at[0, :ROWS, at], x_ref.at[:ROWS, at], w_sems.at[2, k]),
        ])
        for copy in first_pieces[-1]:
            copy.start()
    for step in range(1, seqs * steps):
        s, first = divmod(step * ROWS, span)
        pltpu.make_async_copy(
            x_hbm.at[s, pl.ds(first, ROWS)], x_ref.at[pl.ds(step * ROWS, ROWS)], x_sems.at[step]
        ).start()
    greet(ring, near, me, barrier)
    for s in range(seqs):
        for p in range(pairs):
            q_ref[s * pairs + p : s * pairs + p + 1, :] = probe_ref[s : s + 1, p * LANES : (p + 1) * LANES].astype(F32)

    for copy in gates:
        copy.wait()
    first = lax.axis_index("tp") * heads
    i, j = iotas((16, 2 * all_heads))
    taken = ((i < heads) & (j == first + i)) | ((i >= 8) & (i < 8 + heads) & (j == all_heads + first + i - 8))
    gate_ref[...] = dot(jnp.where(taken, 1.0, 0.0).astype(BF16), wg_ref[...]).astype(BF16)

    def taken_in(copies):
        def wait():
            for copy in copies:
                copy.wait()

        return wait

    refs = (x_ref, w_ref, gate_ref, extra_ref, speed_ref, keys_ref, values_ref, cols_ref, turned_ref)
    project(0, heads, [taken_in(copies) for copies in first_pieces], *refs)
    place, block = lax.rem(me, near), lax.div(me, near)

    def near_copy(pair):
        to, slot = owner(pair)
        return remote(
            tiles.at[pair], near_ref.at[slot, place], send1.at[pair], recv1.at[slot, place], block * near + to
        )

    @pl.loop(0, seqs)
    def _(s):
        @pl.loop(jnp.where(s == 0, 1, 0), steps)
        def _(part):
            step = s * steps + part
            arrival = pltpu.make_async_copy(
                x_hbm.at[0, pl.ds(0, ROWS)], x_ref.at[pl.ds(step * ROWS, ROWS)], x_sems.at[step]
            )
            project(step, heads, [arrival.wait], *refs)

        @pl.when(s == 0)
        def _():
            met(ring, near, me, barrier, ready)

        sequence_maps(
            s, span // CHUNK, heads, keys_ref, values_ref, cols_ref, turned_ref, low_ref, tiles
        )
        for p in range(pairs):
            pair = s * pairs + p

            @pl.when((me > 0) & (place != owner(pair)[0]))
            def _():
                near_copy(pair).start()

    exchange(
        ring, near, me, tiles, near_ref, sent_ref, far_ref, first_ref, rows_ref, final_ref, q_ref,
        (recv1, send2, recv2, send_first, recv_first, send3, recv3, ready),
    )
    for pair in range(near):
        @pl.when((me > 0) & (place != max(pair, 1)))
        def _():
            near_copy(pair).wait_send()

    rows = HEAD // ring
    _, lane = iotas((1, LANES))
    for s in range(seqs):
        for p in range(pairs):
            got = final_ref[s * pairs + p]
            states_ref[s, 2 * p] = got[:rows, :HEAD].astype(BF16)
            states_ref[s, 2 * p + 1] = swapped(got)[:rows, :HEAD].astype(BF16)
            read = got[rows : rows + 1]
            square = read * read
            even = jnp.sum(jnp.where(lane < HEAD, square, 0.0), axis=1, keepdims=True)
            odd = jnp.sum(jnp.where(lane < HEAD, 0.0, square), axis=1, keepdims=True)
            mean = jnp.where(lane < HEAD, even, odd) / HEAD
            reads_ref[s : s + 1, p * LANES : (p + 1) * LANES] = (read * lax.rsqrt(mean + 1e-06)).astype(BF16)


def body(
    ring,
    layer_feed,
    address_mapping,
    content_mapping,
    beta_mapping_matrix,
    forgetting_mapping,
    logged_fading_speed,
    extra_forgetting,
    opening_probe,
):
    seqs, span, depth = layer_feed.shape
    width = address_mapping.shape[1]
    heads = width // HEAD
    all_heads = beta_mapping_matrix.shape[1]
    tokens = seqs * span
    near = seqs * heads // 2
    places = tokens // CHUNK
    chains = span // CHUNK * heads
    hbm = pl.BlockSpec(memory_space=pl.ANY)
    vmem = pl.BlockSpec(memory_space=pltpu.VMEM)
    dma = pltpu.SemaphoreType.DMA
    return pl.pallas_call(
        functools.partial(kernel, ring, heads, all_heads),
        out_shape=(
            jax.ShapeDtypeStruct((seqs, heads, HEAD // ring, HEAD), BF16),
            jax.ShapeDtypeStruct((seqs, width), BF16),
        ),
        in_specs=[hbm] * 5 + [pl.BlockSpec(memory_space=pltpu.SMEM), vmem, vmem],
        out_specs=(vmem, vmem),
        scratch_shapes=[
            pltpu.VMEM((tokens, depth), BF16),
            pltpu.VMEM((depth, 2 * width), BF16),
            pltpu.VMEM((2 * all_heads, depth), BF16),
            pltpu.VMEM((16, depth), BF16),
            pltpu.VMEM((tokens, width), BF16),
            pltpu.VMEM((tokens, width), BF16),
            pltpu.VMEM((places, CHUNK, 16), F32),
            pltpu.VMEM((places, 16, LANES), F32),
            pltpu.VMEM((chains, CHUNK, CHUNK), BF16),
            pltpu.VMEM((near, LANES, LANES), F32),
            pltpu.VMEM((2, near, LANES, LANES), F32),
            pltpu.VMEM((near, LANES, LANES), F32),
            pltpu.VMEM((2, ring // near - 1, LANES, LANES), F32),
            pltpu.VMEM((2, HEAD, LANES), F32),
            pltpu.VMEM((2, ring, 8, LANES), F32),
            pltpu.VMEM((near, 8, LANES), F32),
            pltpu.VMEM((near, LANES), F32),
            dma((2,)),
            dma((3, PIECES)),
            dma((tokens // ROWS,)),
            dma((near,)),
            dma((2, near)),
            dma((2,)),
            dma((2, ring // near - 1)),
            dma((near,)),
            dma((2,)),
            dma((2, ring)),
            dma((near,)),
            pltpu.SemaphoreType.REGULAR,
        ],
        compiler_params=pltpu.CompilerParams(
            collective_id=0, has_side_effects=True, vmem_limit_bytes=56 * 1024 * 1024
        ),
    )(
        layer_feed,
        address_mapping,
        content_mapping,
        beta_mapping_matrix.T,
        forgetting_mapping.T,
        logged_fading_speed,
        extra_forgetting.transpose(0, 2, 1),
        opening_probe,
    )


def solution(mesh):
    in_specs = (
        P("grp", "sp", None),
        P(None, "tp"),
        P(None, "tp"),
        P(),
        P(),
        P("tp"),
        P("grp", "sp", "tp"),
        P("grp", "tp"),
    )
    out_specs = (P("grp", "tp", "sp", None), P("grp", "tp"))
    return jax.shard_map(
        functools.partial(body, mesh.shape["sp"]),
        mesh=mesh,
        in_specs=in_specs,
        out_specs=out_specs,
        check_vma=False,
    )
```

```python
import functools

import jax
import jax.numpy as jnp
from jax import lax
from jax.experimental import pallas as pl
from jax.experimental.pallas import tpu as pltpu
from jax.sharding import PartitionSpec as P

HEAD = 64
LANES = 128
CHUNK = 128
ROWS = 256
PIECES = 4
AHEAD = 3
MESH = pl.DeviceIdType.MESH
F32 = jnp.float32
BF16 = jnp.bfloat16
NN = (((1,), (0,)), ((), ()))
NT = (((1,), (1,)), ((), ()))
TN = (((0,), (0,)), ((), ()))


def dot(left, right, dims=NN):
    return lax.dot_general(left, right, dims, preferred_element_type=F32)


def split(x):
    high = x.astype(BF16)
    return high, (x - high.astype(F32)).astype(BF16)


def matmul(left, right):
    lh, ll = split(left)
    rh, rl = split(right)
    wide = jnp.concatenate(
        [jnp.concatenate([rh, rl], axis=1), jnp.concatenate([rh, jnp.zeros_like(rh)], axis=1)], axis=0
    )
    both = dot(jnp.concatenate([lh, ll], axis=1), wide)
    return both[:, : right.shape[1]] + both[:, right.shape[1] :]


def iotas(shape):
    return lax.broadcasted_iota(jnp.int32, shape, 0), lax.broadcasted_iota(jnp.int32, shape, 1)


def swapped(x):
    return pltpu.roll(x, HEAD, 1)


def diagonal():
    i, j = iotas((LANES, LANES))
    return (i < HEAD) == (j < HEAD)


def composed(later, earlier):
    own = diagonal()
    return matmul(jnp.where(own, swapped(later), 0.0), earlier) + jnp.where(own, later, 0.0)


def silu(x):
    return x / (1.0 + jnp.exp(-x))


def project(step, pieces, x_ref, w_ref, gate_ref, raw_ref, pre_ref):
    rows = pl.ds(step * ROWS, ROWS)
    count = max(len(pieces), 1)
    depth = x_ref.shape[1] // count
    both = pre = None
    for k in range(count):
        if pieces:
            pieces[k]()
        at = slice(k * depth, (k + 1) * depth)
        x = x_ref[rows, at]
        part, gates = dot(x, w_ref[at, :]), dot(gate_ref[:, at], x, NT)
        both, pre = (part, gates) if k == 0 else (both + part, pre + gates)
    raw_ref[rows, :] = both.astype(BF16)
    pre_ref[step] = pre.astype(BF16).astype(F32)


def chunk_parts(
    step, heads, raw_ref, pre_ref, extra_ref, speed_ref, low_ref, inside_ref, start_ref, right_ref, carried_ref, closing_ref
):
    rows = pl.ds(step * ROWS, ROWS)
    width = heads * HEAD
    keys = silu(raw_ref[rows, :width].astype(F32))
    i, j = iotas((width, width))
    same = jnp.where(i // HEAD == j // HEAD, 1.0, 0.0).astype(BF16)
    squares = dot((keys * keys).astype(BF16), same)
    keys = keys * lax.rsqrt(squares + 1e-06)
    values = silu(raw_ref[rows, width:].astype(F32))
    pre = pre_ref[step]

    spans = extra_ref.shape[2] // ROWS
    at = pl.ds(pl.multiple_of(lax.rem(step, spans) * ROWS, ROWS), ROWS)
    extra = extra_ref[lax.div(step, spans), :, at].astype(F32)
    extra = jnp.concatenate([extra, jnp.zeros((8 - heads, ROWS), F32)], axis=0)
    i, _ = iotas((8, ROWS))
    speed = jnp.zeros((8, ROWS), F32)
    for h in range(heads):
        speed = jnp.where(i == h, speed_ref[h], speed)
    betas = 1.0 / (1.0 + jnp.exp(-pre[:8]))
    fade = pre[8:]
    plus = jnp.maximum(fade, 0.0) + jnp.log(1.0 + jnp.exp(-jnp.abs(fade)))
    decay = -jnp.exp(speed) * plus + extra

    i, j = iotas((CHUNK, CHUNK))
    until = jnp.where(i <= j, 1.0, 0.0)
    left = j < HEAD
    left_bf = jnp.where(left, 1.0, 0.0).astype(BF16)
    near = jnp.where((i // SMALL) == (j // SMALL), 1.0, 0.0).astype(BF16)
    r, l = iotas((SMALL, LANES))
    c = l % SMALL
    close = jnp.where(r > c, r ^ c, 0)
    unit = jnp.where(r == c, 1.0, 0.0)
    for part in range(ROWS // CHUNK):
        at = slice(part * CHUNK, (part + 1) * CHUNK)
        totals = lax.dot_general(
            decay[:, at], until, NN, precision=lax.Precision.HIGHEST, preferred_element_type=F32
        )
        mixed = jnp.concatenate([betas[:, at], totals], axis=0)
        cols = jnp.transpose(mixed)
        for p in range(heads // 2):
            pair = slice(p * LANES, (p + 1) * LANES)
            k, v = keys[at, pair], values[at, pair]
            turned = swapped(k)
            kb = k.astype(BF16)
            even = kb * left_bf
            gram = dot(jnp.concatenate([even, kb - even], axis=0), kb, NT)
            for side in range(2):
                h = 2 * p + side
                slot = (step * (ROWS // CHUNK) + part) * heads + h
                mine = left if side == 0 else ~left
                beta = jnp.broadcast_to(cols[:, h : h + 1], (CHUNK, LANES))
                total = jnp.broadcast_to(cols[:, 8 + h : 9 + h], (CHUNK, LANES))
                ahead = jnp.broadcast_to(mixed[8 + h : 9 + h, :], (CHUNK, LANES))
                lower = beta * gram[side * CHUNK : (side + 1) * CHUNK] * jnp.exp(total - ahead)
                lower = jnp.where(i > j, lower, 0.0).astype(BF16)
                low_ref[slot] = lower
                inside = lower * near
                inside_ref[slot] = inside
                packed = inside[:SMALL]
                for b in range(1, CHUNK // SMALL):
                    packed = packed + inside[b * SMALL : (b + 1) * SMALL]
                start_ref[slot] = (unit - jnp.where(close == 1, packed.astype(F32), 0.0)).astype(BF16)
                right_ref[slot] = (beta * jnp.where(mine, v, -jnp.exp(total) * turned)).astype(BF16)
                last = total[CHUNK - 1 :, :]
                carried_ref[slot] = jnp.where(mine, k * jnp.exp(last - total), 0.0).astype(BF16)
                closing_ref[pl.ds(slot, 1), :] = jnp.exp(last)


SMALL = 16


def sequence_maps(s, chunks, heads, low_ref, inside_ref, start_ref, right_ref, carried_ref, closing_ref, tiles):
    first = s * chunks * heads
    slots = range(chunks * heads)
    count = CHUNK // SMALL
    i, j = iotas((CHUNK, CHUNK))
    same = jnp.where((i // SMALL) == (j // SMALL), 1.0, 0.0).astype(BF16)
    apart = jnp.where(i > j, i ^ j, 0)
    r, l = iotas((SMALL, LANES))
    c = l % SMALL
    close = jnp.where(r > c, r ^ c, 0)

    def by_two(lefts, rights):
        out = []
        for n in range(0, len(lefts), 2):
            both = dot(jnp.concatenate(lefts[n : n + 2], axis=0), jnp.concatenate(rights[n : n + 2], axis=1))
            out += [both[:SMALL, :LANES], both[SMALL:, LANES:]]
        return out

    state = [start_ref[first + slot] for slot in slots]
    level = 1
    while 2 << level <= SMALL:
        inner = [y.astype(BF16) for y in by_two(state, [inside_ref[first + slot] for slot in slots])]
        inner = by_two(inner, [jnp.concatenate([x] * count, axis=0) * same for x in state])
        state = [x - jnp.where((close >> level) == 1, y, 0.0).astype(BF16) for x, y in zip(state, inner)]
        level += 1
    state = [jnp.concatenate([x] * count, axis=0) * same for x in state]
    while 2 << level <= CHUNK:
        size = 1 << level
        odd = [slice(b * size, (b + 1) * size) for b in range(1, CHUNK // size, 2)]
        even = [slice(b * size, (b + 1) * size) for b in range(0, CHUNK // size, 2)]
        here = jnp.concatenate([apart[at] for at in odd], axis=0)
        part = [jnp.concatenate([x[at] for at in odd], axis=0) for x in state]
        inner = [dot(x, low_ref[first + slot]).astype(BF16) for slot, x in enumerate(part)]
        inner = [dot(y, x) for y, x in zip(inner, state)]
        part = [x - jnp.where((here >> level) == 1, y, 0.0).astype(BF16) for x, y in zip(part, inner)]
        state = [
            jnp.concatenate(
                [z for b, at in enumerate(even) for z in (x[at], y[b * size : (b + 1) * size])], axis=0
            )
            for x, y in zip(state, part)
        ]
        level += 1
    solved = [dot(x, right_ref[first + slot]).astype(BF16) for slot, x in enumerate(state)]
    for p in range(heads // 2):
        parts = []
        for n in range(chunks):
            slot = n * heads + 2 * p
            carried = jnp.concatenate([carried_ref[first + slot], carried_ref[first + slot + 1]], axis=0)
            tile = dot(carried, jnp.concatenate(solved[slot : slot + 2], axis=0), TN)
            closing = [
                jnp.broadcast_to(closing_ref[pl.ds(first + slot + side, 1), :], tile.shape) for side in range(2)
            ]
            parts.append(tile + jnp.where(j == (i ^ HEAD), jnp.where(i < HEAD, *closing), 0.0))
        while len(parts) > 1:
            parts = [composed(parts[n + 1], parts[n]) for n in range(0, len(parts), 2)]
        tiles[s * (heads // 2) + p] = parts[0]


def remote(src, dst, send, recv, to):
    return pltpu.make_async_remote_copy(
        src_ref=src, dst_ref=dst, send_sem=send, recv_sem=recv, device_id={"sp": to}, device_id_type=MESH
    )


def signal(semaphore, to):
    pl.semaphore_signal(semaphore, inc=1, device_id={"sp": to}, device_id_type=MESH)


def greet(ring, near, me, barrier):
    far = ring // near
    place, block = lax.rem(me, near), lax.div(me, near)
    for k in range(1, near):
        signal(barrier, block * near + lax.rem(place + k, near))

    @pl.when(block < far - 1)
    def _():
        for k in range(near):
            signal(barrier, (far - 1) * near + k)


def met(ring, near, me, barrier, ready):
    far = ring // near
    place, block = lax.rem(me, near), lax.div(me, near)
    pl.semaphore_wait(barrier, jnp.where(block == far - 1, ring - 1, near - 1))

    @pl.when((block == far - 1) & (place > 0))
    def _():
        signal(ready, 0)
        for b in range(far - 1):
            signal(ready, b * near + place)


def owner(pair):
    return jnp.maximum(pair, 1), jnp.where(pair == 0, 1, 0)


def exchange(ring, near, me, tiles, near_ref, sent_ref, far_ref, first_ref, rows_ref, final_ref, probe_ref, sems):
    recv1, send2, recv2, send_first, recv_first, send3, recv3, ready = sems
    far = ring // near
    place, block = lax.rem(me, near), lax.div(me, near)
    own = diagonal()
    i, j = iotas((LANES, LANES))

    firsts = []
    for pair in range(near):
        to, slot = max(pair, 1), int(pair == 0)
        firsts.append(
            remote(
                sent_ref.at[pair, :HEAD], first_ref.at[slot], send_first.at[pair], recv_first.at[slot],
                (far - 1) * near + to,
            )
        )

    @pl.when(me == 0)
    def _():
        for pair in range(near):
            tile = jnp.where(own, tiles[pair], 0.0)
            sent_ref[pair, :HEAD] = tile[:HEAD] + tile[HEAD:]
        pl.semaphore_wait(ready, near - 1)
        for copy in firsts:
            copy.start()

    outs = [
        remote(
            sent_ref.at[slot], far_ref.at[slot, jnp.minimum(block, far - 2)], send2.at[slot],
            recv2.at[slot, jnp.minimum(block, far - 2)], (far - 1) * near + place,
        )
        for slot in range(2)
    ]

    def final_copy(slot, pair, k):
        to = lax.rem(me + k, ring)
        return remote(rows_ref.at[slot, to], final_ref.at[pair], send3.at[slot, k], recv3.at[pair], to)

    @pl.when((block < far - 1) & (place > 0))
    def _():
        pl.semaphore_wait(ready, 1)

    for slot in (1, 0):
        pair = 0 if slot else place

        @pl.when((place == 1) if slot else (place > 0))
        def _():
            near_ref[slot, place] = tiles[pair]

            @pl.when(block == 0)
            def _():
                near_ref[slot, 0] = jnp.where(j == (i ^ HEAD), 1.0, 0.0)

            def arrived(k):
                @pl.when((place != k) & ((block > 0) | (k > 0)))
                def _():
                    remote(tiles.at[0], near_ref.at[slot, k], send2.at[0], recv1.at[slot, k], me).wait_recv()

            arrived(0)
            tile = near_ref[slot, 0]
            for k in range(1, near):
                arrived(k)
                tile = composed(near_ref[slot, k], tile)

            @pl.when(block < far - 1)
            def _():
                sent_ref[slot] = tile
                outs[slot].start()

            @pl.when(block == far - 1)
            def _():
                remote(sent_ref.at[0, :HEAD], first_ref.at[slot], send2.at[0], recv_first.at[slot], me).wait_recv()
                state = first_ref[slot]
                state = jnp.where(own, jnp.concatenate([state, state], axis=0), 0.0)
                for b in range(far - 1):
                    remote(sent_ref.at[0], far_ref.at[slot, b], send2.at[0], recv2.at[slot, b], me).wait_recv()
                    state = composed(far_ref[slot, b], state)
                state = jnp.where(own, composed(tile, state), 0.0)
                both = state[:HEAD] + state[HEAD:]
                rows = HEAD // ring
                read = matmul(jnp.broadcast_to(probe_ref[pl.ds(pair, 1), :], (8, LANES)), state)
                for d in range(ring):
                    rows_ref[slot, d, :rows] = both[d * rows : (d + 1) * rows]
                    rows_ref[slot, d, rows : rows + 1] = read[:1]

                @pl.loop(1, ring)
                def _(k):
                    final_copy(slot, pair, k).start()

                final_ref[pair] = rows_ref[slot, me]

    for pair in range(near):
        @pl.when((block < far - 1) | (place != max(pair, 1)))
        def _():
            remote(rows_ref.at[0, 0], final_ref.at[pair], send3.at[0, 0], recv3.at[pair], me).wait_recv()

    @pl.when(me == 0)
    def _():
        for copy in firsts:
            copy.wait_send()

    for slot in (1, 0):
        active = (place == 1) if slot else (place > 0)

        @pl.when(active & (block < far - 1))
        def _():
            outs[slot].wait_send()

        @pl.when(active & (block == far - 1))
        def _():
            @pl.loop(1, ring)
            def _(k):
                final_copy(slot, 0 if slot else place, k).wait_send()


def kernel(
    ring,
    heads,
    all_heads,
    x_hbm,
    wk_hbm,
    wv_hbm,
    wb_hbm,
    wf_hbm,
    speed_ref,
    extra_ref,
    probe_ref,
    states_ref,
    reads_ref,
    x_ref,
    w_ref,
    wg_ref,
    gate_ref,
    raw_ref,
    pre_ref,
    low_ref,
    inside_ref,
    start_ref,
    right_ref,
    carried_ref,
    closing_ref,
    tiles,
    near_ref,
    sent_ref,
    far_ref,
    first_ref,
    rows_ref,
    final_ref,
    q_ref,
    gate_sems,
    w_sems,
    x_sems,
    send1,
    recv1,
    send2,
    recv2,
    send_first,
    recv_first,
    send3,
    recv3,
    ready,
):
    me = lax.axis_index("sp")
    width = heads * HEAD
    seqs, span, _ = x_hbm.shape
    pairs = heads // 2
    near = seqs * pairs
    far = ring // near
    barrier = pltpu.get_barrier_semaphore()
    gates = [
        pltpu.make_async_copy(wb_hbm, wg_ref.at[:all_heads], gate_sems.at[0]),
        pltpu.make_async_copy(wf_hbm, wg_ref.at[all_heads:], gate_sems.at[1]),
    ]
    for copy in gates:
        copy.start()
    depth = x_hbm.shape[2] // PIECES
    steps = span // ROWS
    first_pieces = []
    for k in range(PIECES):
        at = pl.ds(k * depth, depth)
        first_pieces.append([
            pltpu.make_async_copy(wk_hbm.at[at], w_ref.at[at, :width], w_sems.at[0, k]),
            pltpu.make_async_copy(wv_hbm.at[at], w_ref.at[at, width:], w_sems.at[1, k]),
            pltpu.make_async_copy(x_hbm.at[0, :ROWS, at], x_ref.at[:ROWS, at], w_sems.at[2, k]),
        ])
    later = []
    for step in range(1, seqs * steps):
        s, first = divmod(step * ROWS, span)
        later.append([
            pltpu.make_async_copy(
                x_hbm.at[s, pl.ds(first, ROWS)], x_ref.at[pl.ds(step * ROWS, ROWS)], x_sems.at[step]
            )
        ])
    queue = first_pieces + later
    for copies in queue[:AHEAD]:
        for copy in copies:
            copy.start()
    greet(ring, near, me, barrier)
    for s in range(seqs):
        for p in range(pairs):
            q_ref[s * pairs + p : s * pairs + p + 1, :] = probe_ref[s : s + 1, p * LANES : (p + 1) * LANES].astype(F32)

    for copy in gates:
        copy.wait()
    first = lax.axis_index("tp") * heads
    i, j = iotas((16, 2 * all_heads))
    taken = ((i < heads) & (j == first + i)) | ((i >= 8) & (i < 8 + heads) & (j == all_heads + first + i - 8))
    gate_ref[...] = dot(jnp.where(taken, 1.0, 0.0).astype(BF16), wg_ref[...]).astype(BF16)

    def taken_in(k):
        def wait():
            for copy in queue[k]:
                copy.wait()
            for copies in queue[k + AHEAD : k + AHEAD + 1] if k + 1 < PIECES else queue[k + AHEAD :]:
                for copy in copies:
                    copy.start()

        return wait

    project(0, [taken_in(k) for k in range(PIECES)], x_ref, w_ref, gate_ref, raw_ref, pre_ref)
    parts = (low_ref, inside_ref, start_ref, right_ref, carried_ref, closing_ref)

    @pl.loop(1, seqs * steps)
    def _(step):
        arrival = pltpu.make_async_copy(
            x_hbm.at[0, pl.ds(0, ROWS)], x_ref.at[pl.ds(step * ROWS, ROWS)], x_sems.at[step]
        )
        arrival.wait()
        chunk_parts(step - 1, heads, raw_ref, pre_ref, extra_ref, speed_ref, *parts)
        project(step, [], x_ref, w_ref, gate_ref, raw_ref, pre_ref)

    chunk_parts(seqs * steps - 1, heads, raw_ref, pre_ref, extra_ref, speed_ref, *parts)
    met(ring, near, me, barrier, ready)
    place, block = lax.rem(me, near), lax.div(me, near)

    def near_copy(pair):
        to, slot = owner(pair)
        return remote(
            tiles.at[pair], near_ref.at[slot, place], send1.at[pair], recv1.at[slot, place], block * near + to
        )

    @pl.loop(0, seqs)
    def _(s):
        sequence_maps(s, span // CHUNK, heads, *parts, tiles)
        for p in range(pairs):
            pair = s * pairs + p

            @pl.when((me > 0) & (place != owner(pair)[0]))
            def _():
                near_copy(pair).start()

    exchange(
        ring, near, me, tiles, near_ref, sent_ref, far_ref, first_ref, rows_ref, final_ref, q_ref,
        (recv1, send2, recv2, send_first, recv_first, send3, recv3, ready),
    )
    for pair in range(near):
        @pl.when((me > 0) & (place != max(pair, 1)))
        def _():
            near_copy(pair).wait_send()

    rows = HEAD // ring
    _, lane = iotas((1, LANES))
    for s in range(seqs):
        for p in range(pairs):
            got = final_ref[s * pairs + p]
            states_ref[s, 2 * p] = got[:rows, :HEAD].astype(BF16)
            states_ref[s, 2 * p + 1] = swapped(got)[:rows, :HEAD].astype(BF16)
            read = got[rows : rows + 1]
            square = read * read
            even = jnp.sum(jnp.where(lane < HEAD, square, 0.0), axis=1, keepdims=True)
            odd = jnp.sum(jnp.where(lane < HEAD, 0.0, square), axis=1, keepdims=True)
            mean = jnp.where(lane < HEAD, even, odd) / HEAD
            reads_ref[s : s + 1, p * LANES : (p + 1) * LANES] = (read * lax.rsqrt(mean + 1e-06)).astype(BF16)


def body(
    ring,
    layer_feed,
    address_mapping,
    content_mapping,
    beta_mapping_matrix,
    forgetting_mapping,
    logged_fading_speed,
    extra_forgetting,
    opening_probe,
):
    seqs, span, depth = layer_feed.shape
    width = address_mapping.shape[1]
    heads = width // HEAD
    all_heads = beta_mapping_matrix.shape[1]
    tokens = seqs * span
    near = seqs * heads // 2
    chains = tokens // CHUNK * heads
    hbm = pl.BlockSpec(memory_space=pl.ANY)
    vmem = pl.BlockSpec(memory_space=pltpu.VMEM)
    dma = pltpu.SemaphoreType.DMA
    return pl.pallas_call(
        functools.partial(kernel, ring, heads, all_heads),
        out_shape=(
            jax.ShapeDtypeStruct((seqs, heads, HEAD // ring, HEAD), BF16),
            jax.ShapeDtypeStruct((seqs, width), BF16),
        ),
        in_specs=[hbm] * 5 + [pl.BlockSpec(memory_space=pltpu.SMEM), vmem, vmem],
        out_specs=(vmem, vmem),
        scratch_shapes=[
            pltpu.VMEM((tokens, depth), BF16),
            pltpu.VMEM((depth, 2 * width), BF16),
            pltpu.VMEM((2 * all_heads, depth), BF16),
            pltpu.VMEM((16, depth), BF16),
            pltpu.VMEM((tokens, 2 * width), BF16),
            pltpu.VMEM((tokens // ROWS, 16, ROWS), F32),
            pltpu.VMEM((chains, CHUNK, CHUNK), BF16),
            pltpu.VMEM((chains, CHUNK, CHUNK), BF16),
            pltpu.VMEM((chains, SMALL, CHUNK), BF16),
            pltpu.VMEM((chains, CHUNK, CHUNK), BF16),
            pltpu.VMEM((chains, CHUNK, CHUNK), BF16),
            pltpu.VMEM((chains, LANES), F32),
            pltpu.VMEM((near, LANES, LANES), F32),
            pltpu.VMEM((2, near, LANES, LANES), F32),
            pltpu.VMEM((near, LANES, LANES), F32),
            pltpu.VMEM((2, ring // near - 1, LANES, LANES), F32),
            pltpu.VMEM((2, HEAD, LANES), F32),
            pltpu.VMEM((2, ring, 8, LANES), F32),
            pltpu.VMEM((near, 8, LANES), F32),
            pltpu.VMEM((near, LANES), F32),
            dma((2,)),
            dma((3, PIECES)),
            dma((tokens // ROWS,)),
            dma((near,)),
            dma((2, near)),
            dma((2,)),
            dma((2, ring // near - 1)),
            dma((near,)),
            dma((2,)),
            dma((2, ring)),
            dma((near,)),
            pltpu.SemaphoreType.REGULAR,
        ],
        compiler_params=pltpu.CompilerParams(
            collective_id=0, has_side_effects=True, vmem_limit_bytes=56 * 1024 * 1024
        ),
    )(
        layer_feed,
        address_mapping,
        content_mapping,
        beta_mapping_matrix.T,
        forgetting_mapping.T,
        logged_fading_speed,
        extra_forgetting.transpose(0, 2, 1),
        opening_probe,
    )


def solution(mesh):
    in_specs = (
        P("grp", "sp", None),
        P(None, "tp"),
        P(None, "tp"),
        P(),
        P(),
        P("tp"),
        P("grp", "sp", "tp"),
        P("grp", "tp"),
    )
    out_specs = (P("grp", "tp", "sp", None), P("grp", "tp"))
    return jax.shard_map(
        functools.partial(body, mesh.shape["sp"]),
        mesh=mesh,
        in_specs=in_specs,
        out_specs=out_specs,
        check_vma=False,
    )
```

```python
import functools

import jax
import jax.numpy as jnp
from jax import lax
from jax.experimental import pallas as pl
from jax.experimental.pallas import tpu as pltpu
from jax.sharding import PartitionSpec as P

HEAD = 64
LANES = 128
CHUNK = 128
ROWS = 256
PIECES = 4
AHEAD = 3
MESH = pl.DeviceIdType.MESH
F32 = jnp.float32
BF16 = jnp.bfloat16
NN = (((1,), (0,)), ((), ()))
NT = (((1,), (1,)), ((), ()))
TN = (((0,), (0,)), ((), ()))


def dot(left, right, dims=NN):
    return lax.dot_general(left, right, dims, preferred_element_type=F32)


def split(x):
    high = x.astype(BF16)
    return high, (x - high.astype(F32)).astype(BF16)


def matmul(left, right):
    lh, ll = split(left)
    rh, rl = split(right)
    wide = jnp.concatenate(
        [jnp.concatenate([rh, rl], axis=1), jnp.concatenate([rh, jnp.zeros_like(rh)], axis=1)], axis=0
    )
    both = dot(jnp.concatenate([lh, ll], axis=1), wide)
    return both[:, : right.shape[1]] + both[:, right.shape[1] :]


def iotas(shape):
    return lax.broadcasted_iota(jnp.int32, shape, 0), lax.broadcasted_iota(jnp.int32, shape, 1)


def swapped(x):
    return pltpu.roll(x, HEAD, 1)


def diagonal():
    i, j = iotas((LANES, LANES))
    return (i < HEAD) == (j < HEAD)


def composed(later, earlier):
    own = diagonal()
    return matmul(jnp.where(own, swapped(later), 0.0), earlier) + jnp.where(own, later, 0.0)


def silu(x):
    return x / (1.0 + jnp.exp(-x))


def project(step, pieces, x_ref, w_ref, raw_ref):
    rows = pl.ds(step * ROWS, ROWS)
    count = max(len(pieces), 1)
    depth = x_ref.shape[1] // count
    both = None
    for k in range(count):
        if pieces:
            pieces[k]()
        at = slice(k * depth, (k + 1) * depth)
        part = dot(x_ref[rows, at], w_ref[at, :])
        both = part if k == 0 else both + part
    raw_ref[rows, :] = both.astype(BF16)


def project_gates(step, x_ref, gate_ref, pre_ref):
    pre_ref[step] = dot(gate_ref[...], x_ref[pl.ds(step * ROWS, ROWS), :], NT).astype(BF16).astype(F32)


def chunk_parts(
    step, heads, raw_ref, pre_ref, extra_ref, speed_ref, low_ref, inside_ref, start_ref, right_ref, carried_ref, closing_ref
):
    rows = pl.ds(step * ROWS, ROWS)
    width = heads * HEAD
    keys = silu(raw_ref[rows, :width].astype(F32))
    i, j = iotas((width, width))
    same = jnp.where(i // HEAD == j // HEAD, 1.0, 0.0).astype(BF16)
    squares = dot((keys * keys).astype(BF16), same)
    keys = keys * lax.rsqrt(squares + 1e-06)
    values = silu(raw_ref[rows, width:].astype(F32))
    pre = pre_ref[step]

    spans = extra_ref.shape[2] // ROWS
    at = pl.ds(pl.multiple_of(lax.rem(step, spans) * ROWS, ROWS), ROWS)
    extra = extra_ref[lax.div(step, spans), :, at].astype(F32)
    extra = jnp.concatenate([extra, jnp.zeros((8 - heads, ROWS), F32)], axis=0)
    i, _ = iotas((8, ROWS))
    speed = jnp.zeros((8, ROWS), F32)
    for h in range(heads):
        speed = jnp.where(i == h, speed_ref[h], speed)
    betas = 1.0 / (1.0 + jnp.exp(-pre[:8]))
    fade = pre[8:]
    plus = jnp.maximum(fade, 0.0) + jnp.log(1.0 + jnp.exp(-jnp.abs(fade)))
    decay = -jnp.exp(speed) * plus + extra

    i, j = iotas((CHUNK, CHUNK))
    until = jnp.where(i <= j, 1.0, 0.0)
    left = j < HEAD
    left_bf = jnp.where(left, 1.0, 0.0).astype(BF16)
    near = jnp.where((i // SMALL) == (j // SMALL), 1.0, 0.0).astype(BF16)
    r, l = iotas((SMALL, LANES))
    c = l % SMALL
    close = jnp.where(r > c, r ^ c, 0)
    unit = jnp.where(r == c, 1.0, 0.0)
    for part in range(ROWS // CHUNK):
        at = slice(part * CHUNK, (part + 1) * CHUNK)
        totals = lax.dot_general(
            decay[:, at], until, NN, precision=lax.Precision.HIGHEST, preferred_element_type=F32
        )
        mixed = jnp.concatenate([betas[:, at], totals], axis=0)
        cols = jnp.transpose(mixed)
        for p in range(heads // 2):
            pair = slice(p * LANES, (p + 1) * LANES)
            k, v = keys[at, pair], values[at, pair]
            turned = swapped(k)
            kb = k.astype(BF16)
            even = kb * left_bf
            gram = dot(jnp.concatenate([even, kb - even], axis=0), kb, NT)
            for side in range(2):
                h = 2 * p + side
                slot = (step * (ROWS // CHUNK) + part) * heads + h
                mine = left if side == 0 else ~left
                beta = jnp.broadcast_to(cols[:, h : h + 1], (CHUNK, LANES))
                total = jnp.broadcast_to(cols[:, 8 + h : 9 + h], (CHUNK, LANES))
                ahead = jnp.broadcast_to(mixed[8 + h : 9 + h, :], (CHUNK, LANES))
                lower = beta * gram[side * CHUNK : (side + 1) * CHUNK] * jnp.exp(total - ahead)
                lower = jnp.where(i > j, lower, 0.0).astype(BF16)
                low_ref[slot] = lower
                inside = lower * near
                inside_ref[slot] = inside
                packed = inside[:SMALL]
                for b in range(1, CHUNK // SMALL):
                    packed = packed + inside[b * SMALL : (b + 1) * SMALL]
                start_ref[slot] = (unit - jnp.where(close == 1, packed.astype(F32), 0.0)).astype(BF16)
                right_ref[slot] = (beta * jnp.where(mine, v, -jnp.exp(total) * turned)).astype(BF16)
                last = total[CHUNK - 1 :, :]
                carried_ref[slot] = jnp.where(mine, k * jnp.exp(last - total), 0.0).astype(BF16)
                closing_ref[pl.ds(slot, 1), :] = jnp.exp(last)


SMALL = 16


def small_inverses(s, chunks, heads, inside_ref, start_ref):
    first = s * chunks * heads
    slots = range(chunks * heads)
    count = CHUNK // SMALL
    i, j = iotas((CHUNK, CHUNK))
    same = jnp.where((i // SMALL) == (j // SMALL), 1.0, 0.0).astype(BF16)
    r, l = iotas((SMALL, LANES))
    c = l % SMALL
    close = jnp.where(r > c, r ^ c, 0)

    def by_two(lefts, rights):
        out = []
        for n in range(0, len(lefts), 2):
            both = dot(jnp.concatenate(lefts[n : n + 2], axis=0), jnp.concatenate(rights[n : n + 2], axis=1))
            out += [both[:SMALL, :LANES], both[SMALL:, LANES:]]
        return out

    state = [start_ref[first + slot] for slot in slots]
    level = 1
    while 2 << level <= SMALL:
        inner = [y.astype(BF16) for y in by_two(state, [inside_ref[first + slot] for slot in slots])]
        inner = by_two(inner, [jnp.concatenate([x] * count, axis=0) * same for x in state])
        state = [x - jnp.where((close >> level) == 1, y, 0.0).astype(BF16) for x, y in zip(state, inner)]
        level += 1
    return [jnp.concatenate([x] * count, axis=0) * same for x in state]


def sequence_maps(s, chunks, heads, state, low_ref, right_ref, carried_ref, closing_ref, tiles):
    first = s * chunks * heads
    i, j = iotas((CHUNK, CHUNK))
    apart = jnp.where(i > j, i ^ j, 0)
    level = SMALL.bit_length() - 1
    while 2 << level <= CHUNK:
        size = 1 << level
        odd = [slice(b * size, (b + 1) * size) for b in range(1, CHUNK // size, 2)]
        even = [slice(b * size, (b + 1) * size) for b in range(0, CHUNK // size, 2)]
        here = jnp.concatenate([apart[at] for at in odd], axis=0)
        part = [jnp.concatenate([x[at] for at in odd], axis=0) for x in state]
        inner = [dot(x, low_ref[first + slot]).astype(BF16) for slot, x in enumerate(part)]
        inner = [dot(y, x) for y, x in zip(inner, state)]
        part = [x - jnp.where((here >> level) == 1, y, 0.0).astype(BF16) for x, y in zip(part, inner)]
        state = [
            jnp.concatenate(
                [z for b, at in enumerate(even) for z in (x[at], y[b * size : (b + 1) * size])], axis=0
            )
            for x, y in zip(state, part)
        ]
        level += 1
    solved = [dot(x, right_ref[first + slot]).astype(BF16) for slot, x in enumerate(state)]
    for p in range(heads // 2):
        parts = []
        for n in range(chunks):
            slot = n * heads + 2 * p
            carried = jnp.concatenate([carried_ref[first + slot], carried_ref[first + slot + 1]], axis=0)
            tile = dot(carried, jnp.concatenate(solved[slot : slot + 2], axis=0), TN)
            closing = [
                jnp.broadcast_to(closing_ref[pl.ds(first + slot + side, 1), :], tile.shape) for side in range(2)
            ]
            parts.append(tile + jnp.where(j == (i ^ HEAD), jnp.where(i < HEAD, *closing), 0.0))
        while len(parts) > 1:
            parts = [composed(parts[n + 1], parts[n]) for n in range(0, len(parts), 2)]
        tiles[s * (heads // 2) + p] = parts[0]


def remote(src, dst, send, recv, to):
    return pltpu.make_async_remote_copy(
        src_ref=src, dst_ref=dst, send_sem=send, recv_sem=recv, device_id={"sp": to}, device_id_type=MESH
    )


def signal(semaphore, to):
    pl.semaphore_signal(semaphore, inc=1, device_id={"sp": to}, device_id_type=MESH)


def greet(ring, near, me, barrier):
    far = ring // near
    place, block = lax.rem(me, near), lax.div(me, near)
    for k in range(1, near):
        signal(barrier, block * near + lax.rem(place + k, near))

    @pl.when(block < far - 1)
    def _():
        for k in range(near):
            signal(barrier, (far - 1) * near + k)


def met(ring, near, me, barrier, ready):
    far = ring // near
    place, block = lax.rem(me, near), lax.div(me, near)
    pl.semaphore_wait(barrier, jnp.where(block == far - 1, ring - 1, near - 1))

    @pl.when((block == far - 1) & (place > 0))
    def _():
        signal(ready, 0)
        for b in range(far - 1):
            signal(ready, b * near + place)


def exchange(ring, near, me, tiles, near_ref, sent_ref, far_ref, first_ref, rows_ref, final_ref, probe_ref, sems):
    recv1, send2, recv2, send_first, recv_first, send3, recv3, ready = sems
    far = ring // near
    place, block = lax.rem(me, near), lax.div(me, near)
    own = diagonal()
    i, j = iotas((LANES, LANES))

    firsts = []
    for pair in range(near):
        to, slot = max(pair, 1), int(pair == 0)
        firsts.append(
            remote(
                sent_ref.at[pair, :HEAD], first_ref.at[slot], send_first.at[pair], recv_first.at[slot],
                (far - 1) * near + to,
            )
        )

    @pl.when(me == 0)
    def _():
        for pair in range(near):
            tile = jnp.where(own, tiles[pair], 0.0)
            sent_ref[pair, :HEAD] = tile[:HEAD] + tile[HEAD:]
        pl.semaphore_wait(ready, near - 1)
        for copy in firsts:
            copy.start()

    outs = [
        remote(
            sent_ref.at[slot], far_ref.at[slot, jnp.minimum(block, far - 2)], send2.at[slot],
            recv2.at[slot, jnp.minimum(block, far - 2)], (far - 1) * near + place,
        )
        for slot in range(2)
    ]

    def final_copy(slot, pair, k):
        to = lax.rem(me + k, ring)
        return remote(rows_ref.at[slot, to], final_ref.at[pair], send3.at[slot, k], recv3.at[pair], to)

    @pl.when((block < far - 1) & (place > 0))
    def _():
        pl.semaphore_wait(ready, 1)

    for slot in (1, 0):
        pair = 0 if slot else place

        @pl.when((place == 1) if slot else (place > 0))
        def _():
            near_ref[slot, place] = tiles[pair]

            @pl.when(block == 0)
            def _():
                near_ref[slot, 0] = jnp.where(j == (i ^ HEAD), 1.0, 0.0)

            def arrived(k):
                @pl.when((place != k) & ((block > 0) | (k > 0)))
                def _():
                    remote(tiles.at[0], near_ref.at[slot, k], send2.at[0], recv1.at[slot, k], me).wait_recv()

            arrived(0)
            tile = near_ref[slot, 0]
            for k in range(1, near):
                arrived(k)
                tile = composed(near_ref[slot, k], tile)

            @pl.when(block < far - 1)
            def _():
                sent_ref[slot] = tile
                outs[slot].start()

            @pl.when(block == far - 1)
            def _():
                remote(sent_ref.at[0, :HEAD], first_ref.at[slot], send2.at[0], recv_first.at[slot], me).wait_recv()
                state = first_ref[slot]
                state = jnp.where(own, jnp.concatenate([state, state], axis=0), 0.0)
                for b in range(far - 1):
                    remote(sent_ref.at[0], far_ref.at[slot, b], send2.at[0], recv2.at[slot, b], me).wait_recv()
                    state = composed(far_ref[slot, b], state)
                state = jnp.where(own, composed(tile, state), 0.0)
                both = state[:HEAD] + state[HEAD:]
                rows = HEAD // ring
                read = matmul(jnp.broadcast_to(probe_ref[pl.ds(pair, 1), :], (8, LANES)), state)
                for d in range(ring):
                    rows_ref[slot, d, :rows] = both[d * rows : (d + 1) * rows]
                    rows_ref[slot, d, rows : rows + 1] = read[:1]

                @pl.loop(1, ring)
                def _(k):
                    final_copy(slot, pair, k).start()

                final_ref[pair] = rows_ref[slot, me]

    for pair in range(near):
        @pl.when((block < far - 1) | (place != max(pair, 1)))
        def _():
            remote(rows_ref.at[0, 0], final_ref.at[pair], send3.at[0, 0], recv3.at[pair], me).wait_recv()

    @pl.when(me == 0)
    def _():
        for copy in firsts:
            copy.wait_send()

    for slot in (1, 0):
        active = (place == 1) if slot else (place > 0)

        @pl.when(active & (block < far - 1))
        def _():
            outs[slot].wait_send()

        @pl.when(active & (block == far - 1))
        def _():
            @pl.loop(1, ring)
            def _(k):
                final_copy(slot, 0 if slot else place, k).wait_send()


def kernel(
    ring,
    heads,
    all_heads,
    x_hbm,
    wk_hbm,
    wv_hbm,
    wb_hbm,
    wf_hbm,
    speed_hbm,
    extra_hbm,
    probe_hbm,
    states_ref,
    reads_ref,
    speed_ref,
    extra_ref,
    probe_ref,
    x_ref,
    w_ref,
    wg_ref,
    gate_ref,
    raw_ref,
    pre_ref,
    low_ref,
    inside_ref,
    start_ref,
    right_ref,
    carried_ref,
    closing_ref,
    tiles,
    near_ref,
    sent_ref,
    far_ref,
    first_ref,
    rows_ref,
    final_ref,
    q_ref,
    gate_sems,
    w_sems,
    x_sems,
    send1,
    recv1,
    send2,
    recv2,
    send_first,
    recv_first,
    send3,
    recv3,
    ready,
):
    me = lax.axis_index("sp")
    width = heads * HEAD
    seqs, span, _ = x_hbm.shape
    pairs = heads // 2
    near = seqs * pairs
    far = ring // near
    barrier = pltpu.get_barrier_semaphore()
    gates = [
        pltpu.make_async_copy(wb_hbm, wg_ref.at[:all_heads], gate_sems.at[0]),
        pltpu.make_async_copy(wf_hbm, wg_ref.at[all_heads:], gate_sems.at[1]),
        pltpu.make_async_copy(extra_hbm, extra_ref, gate_sems.at[2]),
        pltpu.make_async_copy(probe_hbm, probe_ref, gate_sems.at[3]),
        pltpu.make_async_copy(speed_hbm, speed_ref, gate_sems.at[4]),
    ]
    depth = x_hbm.shape[2] // PIECES
    steps = span // ROWS
    first_pieces = []
    for k in range(PIECES):
        at = pl.ds(k * depth, depth)
        first_pieces.append([
            pltpu.make_async_copy(wk_hbm.at[at], w_ref.at[at, :width], w_sems.at[0, k]),
            pltpu.make_async_copy(wv_hbm.at[at], w_ref.at[at, width:], w_sems.at[1, k]),
            pltpu.make_async_copy(x_hbm.at[0, :ROWS, at], x_ref.at[:ROWS, at], w_sems.at[2, k]),
        ])
    later = []
    for step in range(1, seqs * steps):
        s, first = divmod(step * ROWS, span)
        later.append([
            pltpu.make_async_copy(
                x_hbm.at[s, pl.ds(first, ROWS)], x_ref.at[pl.ds(step * ROWS, ROWS)], x_sems.at[step]
            )
        ])
    queue = first_pieces + later
    for n, copies in enumerate(queue[:AHEAD]):
        for copy in copies:
            copy.start()
        if n == 0:
            for copy in gates:
                copy.start()
    greet(ring, near, me, barrier)

    def taken_in(k):
        def wait():
            for copy in queue[k]:
                copy.wait()
            for copies in queue[k + AHEAD : k + AHEAD + 1] if k + 1 < PIECES else queue[k + AHEAD :]:
                for copy in copies:
                    copy.start()

        return wait

    project(0, [taken_in(k) for k in range(PIECES)], x_ref, w_ref, raw_ref)

    for copy in gates:
        copy.wait()
    first = lax.axis_index("tp") * heads
    i, j = iotas((16, 2 * all_heads))
    taken = ((i < heads) & (j == first + i)) | ((i >= 8) & (i < 8 + heads) & (j == all_heads + first + i - 8))
    gate_ref[...] = dot(jnp.where(taken, 1.0, 0.0).astype(BF16), wg_ref[...]).astype(BF16)
    project_gates(0, x_ref, gate_ref, pre_ref)
    for s in range(seqs):
        for p in range(pairs):
            q_ref[s * pairs + p : s * pairs + p + 1, :] = probe_ref[s : s + 1, p * LANES : (p + 1) * LANES].astype(F32)
    parts = (low_ref, inside_ref, start_ref, right_ref, carried_ref, closing_ref)
    total = seqs * steps

    @pl.loop(1, total)
    def _(step):
        arrival = pltpu.make_async_copy(
            x_hbm.at[0, pl.ds(0, ROWS)], x_ref.at[pl.ds(step * ROWS, ROWS)], x_sems.at[step]
        )
        arrival.wait()
        chunk_parts(step - 1, heads, raw_ref, pre_ref, extra_ref, speed_ref, *parts)
        project(step, [], x_ref, w_ref, raw_ref)
        project_gates(step, x_ref, gate_ref, pre_ref)

    met(ring, near, me, barrier, ready)
    place, block = lax.rem(me, near), lax.div(me, near)

    def near_copy(pair):
        to, slot = max(pair, 1), int(pair == 0)
        return remote(
            tiles.at[pair], near_ref.at[slot, place], send1.at[pair], recv1.at[slot, place], block * near + to
        )

    chunks = span // CHUNK
    chunk_parts(total - 1, heads, raw_ref, pre_ref, extra_ref, speed_ref, *parts)
    state = small_inverses(0, chunks, heads, inside_ref, start_ref)
    for s in range(seqs):
        if s + 1 < seqs:
            following = small_inverses(s + 1, chunks, heads, inside_ref, start_ref)
            for slot, x in enumerate(following):
                inside_ref[(s + 1) * chunks * heads + slot] = x
        sequence_maps(s, chunks, heads, state, low_ref, right_ref, carried_ref, closing_ref, tiles)
        for p in range(pairs):
            pair = s * pairs + p

            @pl.when((me > 0) & (place != max(pair, 1)))
            def _():
                near_copy(pair).start()

        if s + 1 < seqs:
            state = [inside_ref[(s + 1) * chunks * heads + slot] for slot in range(chunks * heads)]

    exchange(
        ring, near, me, tiles, near_ref, sent_ref, far_ref, first_ref, rows_ref, final_ref, q_ref,
        (recv1, send2, recv2, send_first, recv_first, send3, recv3, ready),
    )
    for pair in range(near):
        @pl.when((me > 0) & (place != max(pair, 1)))
        def _():
            near_copy(pair).wait_send()

    rows = HEAD // ring
    _, lane = iotas((1, LANES))
    for s in range(seqs):
        for p in range(pairs):
            got = final_ref[s * pairs + p]
            states_ref[s, 2 * p] = got[:rows, :HEAD].astype(BF16)
            states_ref[s, 2 * p + 1] = swapped(got)[:rows, :HEAD].astype(BF16)
            read = got[rows : rows + 1]
            square = read * read
            even = jnp.sum(jnp.where(lane < HEAD, square, 0.0), axis=1, keepdims=True)
            odd = jnp.sum(jnp.where(lane < HEAD, 0.0, square), axis=1, keepdims=True)
            mean = jnp.where(lane < HEAD, even, odd) / HEAD
            reads_ref[s : s + 1, p * LANES : (p + 1) * LANES] = (read * lax.rsqrt(mean + 1e-06)).astype(BF16)


def body(
    ring,
    layer_feed,
    address_mapping,
    content_mapping,
    beta_mapping_matrix,
    forgetting_mapping,
    logged_fading_speed,
    extra_forgetting,
    opening_probe,
):
    seqs, span, depth = layer_feed.shape
    width = address_mapping.shape[1]
    heads = width // HEAD
    all_heads = beta_mapping_matrix.shape[1]
    tokens = seqs * span
    near = seqs * heads // 2
    chains = tokens // CHUNK * heads
    hbm = pl.BlockSpec(memory_space=pl.ANY)
    vmem = pl.BlockSpec(memory_space=pltpu.VMEM)
    dma = pltpu.SemaphoreType.DMA
    return pl.pallas_call(
        functools.partial(kernel, ring, heads, all_heads),
        out_shape=(
            jax.ShapeDtypeStruct((seqs, heads, HEAD // ring, HEAD), BF16),
            jax.ShapeDtypeStruct((seqs, width), BF16),
        ),
        in_specs=[hbm] * 8,
        out_specs=(vmem, vmem),
        scratch_shapes=[
            pltpu.SMEM((heads,), F32),
            pltpu.VMEM((seqs, heads, span), BF16),
            pltpu.VMEM((seqs, width), BF16),
            pltpu.VMEM((tokens, depth), BF16),
            pltpu.VMEM((depth, 2 * width), BF16),
            pltpu.VMEM((2 * all_heads, depth), BF16),
            pltpu.VMEM((16, depth), BF16),
            pltpu.VMEM((tokens, 2 * width), BF16),
            pltpu.VMEM((tokens // ROWS, 16, ROWS), F32),
            pltpu.VMEM((chains, CHUNK, CHUNK), BF16),
            pltpu.VMEM((chains, CHUNK, CHUNK), BF16),
            pltpu.VMEM((chains, SMALL, CHUNK), BF16),
            pltpu.VMEM((chains, CHUNK, CHUNK), BF16),
            pltpu.VMEM((chains, CHUNK, CHUNK), BF16),
            pltpu.VMEM((chains, LANES), F32),
            pltpu.VMEM((near, LANES, LANES), F32),
            pltpu.VMEM((2, near, LANES, LANES), F32),
            pltpu.VMEM((near, LANES, LANES), F32),
            pltpu.VMEM((2, ring // near - 1, LANES, LANES), F32),
            pltpu.VMEM((2, HEAD, LANES), F32),
            pltpu.VMEM((2, ring, 8, LANES), F32),
            pltpu.VMEM((near, 8, LANES), F32),
            pltpu.VMEM((near, LANES), F32),
            dma((5,)),
            dma((3, PIECES)),
            dma((tokens // ROWS,)),
            dma((near,)),
            dma((2, near)),
            dma((2,)),
            dma((2, ring // near - 1)),
            dma((near,)),
            dma((2,)),
            dma((2, ring)),
            dma((near,)),
            pltpu.SemaphoreType.REGULAR,
        ],
        compiler_params=pltpu.CompilerParams(
            collective_id=0, has_side_effects=True, vmem_limit_bytes=56 * 1024 * 1024
        ),
    )(
        layer_feed,
        address_mapping,
        content_mapping,
        beta_mapping_matrix.T,
        forgetting_mapping.T,
        logged_fading_speed,
        extra_forgetting.transpose(0, 2, 1),
        opening_probe,
    )


def solution(mesh):
    in_specs = (
        P("grp", "sp", None),
        P(None, "tp"),
        P(None, "tp"),
        P(),
        P(),
        P("tp"),
        P("grp", "sp", "tp"),
        P("grp", "tp"),
    )
    out_specs = (P("grp", "tp", "sp", None), P("grp", "tp"))
    return jax.shard_map(
        functools.partial(body, mesh.shape["sp"]),
        mesh=mesh,
        in_specs=in_specs,
        out_specs=out_specs,
        check_vma=False,
    )
```

```python
import functools

import jax
import jax.numpy as jnp
from jax import lax
from jax.experimental import pallas as pl
from jax.experimental.pallas import tpu as pltpu
from jax.sharding import PartitionSpec as P

HEAD = 64
LANES = 128
CHUNK = 128
ROWS = 256
PIECES = 4
AHEAD = 3
MESH = pl.DeviceIdType.MESH
F32 = jnp.float32
BF16 = jnp.bfloat16
NN = (((1,), (0,)), ((), ()))
NT = (((1,), (1,)), ((), ()))
TN = (((0,), (0,)), ((), ()))


def dot(left, right, dims=NN):
    return lax.dot_general(left, right, dims, preferred_element_type=F32)


def split(x):
    high = x.astype(BF16)
    return high, (x - high.astype(F32)).astype(BF16)


def matmul(left, right):
    lh, ll = split(left)
    rh, rl = split(right)
    wide = jnp.concatenate(
        [jnp.concatenate([rh, rl], axis=1), jnp.concatenate([rh, jnp.zeros_like(rh)], axis=1)], axis=0
    )
    both = dot(jnp.concatenate([lh, ll], axis=1), wide)
    return both[:, : right.shape[1]] + both[:, right.shape[1] :]


def iotas(shape):
    return lax.broadcasted_iota(jnp.int32, shape, 0), lax.broadcasted_iota(jnp.int32, shape, 1)


def swapped(x):
    return pltpu.roll(x, HEAD, 1)


def diagonal():
    i, j = iotas((LANES, LANES))
    return (i < HEAD) == (j < HEAD)


def composed(later, earlier):
    own = diagonal()
    return matmul(jnp.where(own, swapped(later), 0.0), earlier) + jnp.where(own, later, 0.0)


def silu(x):
    return x / (1.0 + jnp.exp(-x))


def project(step, pieces, x_ref, w_ref, raw_ref):
    rows = pl.ds(step * ROWS, ROWS)
    count = max(len(pieces), 1)
    depth = x_ref.shape[1] // count
    both = None
    for k in range(count):
        if pieces:
            pieces[k]()
        at = slice(k * depth, (k + 1) * depth)
        part = dot(x_ref[rows, at], w_ref[at, :])
        both = part if k == 0 else both + part
    raw_ref[rows, :] = both.astype(BF16)


def project_gates(step, x_ref, gate_ref, pre_ref):
    pre_ref[step] = dot(gate_ref[...], x_ref[pl.ds(step * ROWS, ROWS), :], NT).astype(BF16).astype(F32)


def chunk_parts(
    step, heads, raw_ref, pre_ref, extra_ref, speed_ref, low_ref, inside_ref, start_ref, right_ref, carried_ref, closing_ref
):
    rows = pl.ds(step * ROWS, ROWS)
    width = heads * HEAD
    keys = silu(raw_ref[rows, :width].astype(F32))
    i, j = iotas((width, width))
    same = jnp.where(i // HEAD == j // HEAD, 1.0, 0.0).astype(BF16)
    squares = dot((keys * keys).astype(BF16), same)
    keys = keys * lax.rsqrt(squares + 1e-06)
    values = silu(raw_ref[rows, width:].astype(F32))
    pre = pre_ref[step]

    spans = extra_ref.shape[2] // ROWS
    at = pl.ds(pl.multiple_of(lax.rem(step, spans) * ROWS, ROWS), ROWS)
    extra = extra_ref[lax.div(step, spans), :, at].astype(F32)
    extra = jnp.concatenate([extra, jnp.zeros((8 - heads, ROWS), F32)], axis=0)
    i, _ = iotas((8, ROWS))
    speed = jnp.zeros((8, ROWS), F32)
    for h in range(heads):
        speed = jnp.where(i == h, speed_ref[h], speed)
    betas = 1.0 / (1.0 + jnp.exp(-pre[:8]))
    fade = pre[8:]
    plus = jnp.maximum(fade, 0.0) + jnp.log(1.0 + jnp.exp(-jnp.abs(fade)))
    decay = -jnp.exp(speed) * plus + extra

    i, j = iotas((CHUNK, CHUNK))
    until = jnp.where(i <= j, 1.0, 0.0)
    left = j < HEAD
    left_bf = jnp.where(left, 1.0, 0.0).astype(BF16)
    near = jnp.where((i // SMALL) == (j // SMALL), 1.0, 0.0).astype(BF16)
    r, l = iotas((SMALL, LANES))
    c = l % SMALL
    close = jnp.where(r > c, r ^ c, 0)
    unit = jnp.where(r == c, 1.0, 0.0)
    for part in range(ROWS // CHUNK):
        at = slice(part * CHUNK, (part + 1) * CHUNK)
        totals = lax.dot_general(
            decay[:, at], until, NN, precision=lax.Precision.HIGHEST, preferred_element_type=F32
        )
        mixed = jnp.concatenate([betas[:, at], totals], axis=0)
        cols = jnp.transpose(mixed)
        for p in range(heads // 2):
            pair = slice(p * LANES, (p + 1) * LANES)
            k, v = keys[at, pair], values[at, pair]
            turned = swapped(k)
            kb = k.astype(BF16)
            even = kb * left_bf
            gram = dot(jnp.concatenate([even, kb - even], axis=0), kb, NT)
            for side in range(2):
                h = 2 * p + side
                slot = (step * (ROWS // CHUNK) + part) * heads + h
                mine = left if side == 0 else ~left
                beta = jnp.broadcast_to(cols[:, h : h + 1], (CHUNK, LANES))
                total = jnp.broadcast_to(cols[:, 8 + h : 9 + h], (CHUNK, LANES))
                ahead = jnp.broadcast_to(mixed[8 + h : 9 + h, :], (CHUNK, LANES))
                lower = beta * gram[side * CHUNK : (side + 1) * CHUNK] * jnp.exp(total - ahead)
                lower = jnp.where(i > j, lower, 0.0).astype(BF16)
                low_ref[slot] = lower
                inside = lower * near
                inside_ref[slot] = inside
                packed = inside[:SMALL]
                for b in range(1, CHUNK // SMALL):
                    packed = packed + inside[b * SMALL : (b + 1) * SMALL]
                start_ref[slot] = (unit - jnp.where(close == 1, packed.astype(F32), 0.0)).astype(BF16)
                right_ref[slot] = (beta * jnp.where(mine, v, -jnp.exp(total) * turned)).astype(BF16)
                last = total[CHUNK - 1 :, :]
                carried_ref[slot] = jnp.where(mine, k * jnp.exp(last - total), 0.0).astype(BF16)
                closing_ref[pl.ds(slot, 1), :] = jnp.exp(last)


SMALL = 16


def small_inverses(s, chunks, heads, inside_ref, start_ref):
    first = s * chunks * heads
    slots = range(chunks * heads)
    count = CHUNK // SMALL
    i, j = iotas((CHUNK, CHUNK))
    same = jnp.where((i // SMALL) == (j // SMALL), 1.0, 0.0).astype(BF16)
    r, l = iotas((SMALL, LANES))
    c = l % SMALL
    close = jnp.where(r > c, r ^ c, 0)

    def by_two(lefts, rights):
        out = []
        for n in range(0, len(lefts), 2):
            both = dot(jnp.concatenate(lefts[n : n + 2], axis=0), jnp.concatenate(rights[n : n + 2], axis=1))
            out += [both[:SMALL, :LANES], both[SMALL:, LANES:]]
        return out

    state = [start_ref[first + slot] for slot in slots]
    level = 1
    while 2 << level <= SMALL:
        inner = [y.astype(BF16) for y in by_two(state, [inside_ref[first + slot] for slot in slots])]
        inner = by_two(inner, [jnp.concatenate([x] * count, axis=0) * same for x in state])
        state = [x - jnp.where((close >> level) == 1, y, 0.0).astype(BF16) for x, y in zip(state, inner)]
        level += 1
    return [jnp.concatenate([x] * count, axis=0) * same for x in state]


def sequence_maps(s, chunks, heads, state, low_ref, right_ref, carried_ref, closing_ref, tiles):
    first = s * chunks * heads
    i, j = iotas((CHUNK, CHUNK))
    apart = jnp.where(i > j, i ^ j, 0)
    level = SMALL.bit_length() - 1
    while 2 << level <= CHUNK:
        size = 1 << level
        odd = [slice(b * size, (b + 1) * size) for b in range(1, CHUNK // size, 2)]
        even = [slice(b * size, (b + 1) * size) for b in range(0, CHUNK // size, 2)]
        here = jnp.concatenate([apart[at] for at in odd], axis=0)
        part = [jnp.concatenate([x[at] for at in odd], axis=0) for x in state]
        inner = [dot(x, low_ref[first + slot]).astype(BF16) for slot, x in enumerate(part)]
        inner = [dot(y, x) for y, x in zip(inner, state)]
        part = [x - jnp.where((here >> level) == 1, y, 0.0).astype(BF16) for x, y in zip(part, inner)]
        state = [
            jnp.concatenate(
                [z for b, at in enumerate(even) for z in (x[at], y[b * size : (b + 1) * size])], axis=0
            )
            for x, y in zip(state, part)
        ]
        level += 1
    solved = [dot(x, right_ref[first + slot]).astype(BF16) for slot, x in enumerate(state)]
    for p in range(heads // 2):
        parts = []
        for n in range(chunks):
            slot = n * heads + 2 * p
            carried = jnp.concatenate([carried_ref[first + slot], carried_ref[first + slot + 1]], axis=0)
            tile = dot(carried, jnp.concatenate(solved[slot : slot + 2], axis=0), TN)
            closing = [
                jnp.broadcast_to(closing_ref[pl.ds(first + slot + side, 1), :], tile.shape) for side in range(2)
            ]
            parts.append(tile + jnp.where(j == (i ^ HEAD), jnp.where(i < HEAD, *closing), 0.0))
        while len(parts) > 1:
            parts = [composed(parts[n + 1], parts[n]) for n in range(0, len(parts), 2)]
        tiles[s * (heads // 2) + p] = parts[0]


def remote(src, dst, send, recv, to):
    return pltpu.make_async_remote_copy(
        src_ref=src, dst_ref=dst, send_sem=send, recv_sem=recv, device_id={"sp": to}, device_id_type=MESH
    )


def signal(semaphore, to):
    pl.semaphore_signal(semaphore, inc=1, device_id={"sp": to}, device_id_type=MESH)


def greet(ring, near, me, barrier):
    far = ring // near
    place, block = lax.rem(me, near), lax.div(me, near)
    for k in range(1, near):
        to = block * near + lax.rem(place + k, near)

        @pl.when((me > 0) & (to > 0))
        def _():
            signal(barrier, to)

    @pl.when(block < far - 1)
    def _():
        for k in range(near):
            signal(barrier, (far - 1) * near + k)


def met(ring, near, me, barrier, ready):
    far = ring // near
    place, block = lax.rem(me, near), lax.div(me, near)
    count = jnp.where(block == far - 1, ring - 1, jnp.where(block == 0, near - 2, near - 1))

    @pl.when(me > 0)
    def _():
        pl.semaphore_wait(barrier, count)

    @pl.when((block == far - 1) & (place > 0))
    def _():
        signal(ready, 0)
        for b in range(far - 1):
            signal(ready, b * near + place)


def exchange(ring, near, me, tiles, near_ref, sent_ref, far_ref, first_ref, rows_ref, final_ref, probe_ref, sems):
    recv1, send2, recv2, send_first, recv_first, send3, recv3, ready = sems
    far = ring // near
    place, block = lax.rem(me, near), lax.div(me, near)
    own = diagonal()
    i, j = iotas((LANES, LANES))

    firsts = []
    for pair in range(near):
        to, slot = max(pair, 1), int(pair == 0)
        firsts.append(
            remote(
                sent_ref.at[pair, :HEAD], first_ref.at[slot], send_first.at[pair], recv_first.at[slot],
                (far - 1) * near + to,
            )
        )

    @pl.when(me == 0)
    def _():
        for pair in range(near):
            tile = jnp.where(own, tiles[pair], 0.0)
            sent_ref[pair, :HEAD] = tile[:HEAD] + tile[HEAD:]
        pl.semaphore_wait(ready, near - 1)
        for copy in firsts:
            copy.start()

    outs = [
        remote(
            sent_ref.at[slot], far_ref.at[slot, jnp.minimum(block, far - 2)], send2.at[slot],
            recv2.at[slot, jnp.minimum(block, far - 2)], (far - 1) * near + place,
        )
        for slot in range(2)
    ]

    def final_copy(slot, pair, k):
        to = lax.rem(me + k, ring)
        return remote(rows_ref.at[slot, to], final_ref.at[pair], send3.at[slot, k], recv3.at[pair], to)

    @pl.when((block < far - 1) & (place > 0))
    def _():
        pl.semaphore_wait(ready, 1)

    for slot in (1, 0):
        pair = 0 if slot else place

        @pl.when((place == 1) if slot else (place > 0))
        def _():
            near_ref[slot, place] = tiles[pair]

            @pl.when(block == 0)
            def _():
                near_ref[slot, 0] = jnp.where(j == (i ^ HEAD), 1.0, 0.0)

            def arrived(k):
                @pl.when((place != k) & ((block > 0) | (k > 0)))
                def _():
                    remote(tiles.at[0], near_ref.at[slot, k], send2.at[0], recv1.at[slot, k], me).wait_recv()

            arrived(0)
            tile = near_ref[slot, 0]
            for k in range(1, near):
                arrived(k)
                tile = composed(near_ref[slot, k], tile)

            @pl.when(block < far - 1)
            def _():
                sent_ref[slot] = tile
                outs[slot].start()

            @pl.when(block == far - 1)
            def _():
                remote(sent_ref.at[0, :HEAD], first_ref.at[slot], send2.at[0], recv_first.at[slot], me).wait_recv()
                state = first_ref[slot]
                state = jnp.where(own, jnp.concatenate([state, state], axis=0), 0.0)
                for b in range(far - 1):
                    remote(sent_ref.at[0], far_ref.at[slot, b], send2.at[0], recv2.at[slot, b], me).wait_recv()
                    state = composed(far_ref[slot, b], state)
                state = jnp.where(own, composed(tile, state), 0.0)
                both = state[:HEAD] + state[HEAD:]
                rows = HEAD // ring
                read = matmul(jnp.broadcast_to(probe_ref[pl.ds(pair, 1), :], (8, LANES)), state)
                for d in range(ring):
                    rows_ref[slot, d, :rows] = both[d * rows : (d + 1) * rows]
                    rows_ref[slot, d, rows : rows + 1] = read[:1]

                @pl.loop(1, ring)
                def _(k):
                    final_copy(slot, pair, k).start()

                final_ref[pair] = rows_ref[slot, me]

    for pair in range(near):
        @pl.when((block < far - 1) | (place != max(pair, 1)))
        def _():
            remote(rows_ref.at[0, 0], final_ref.at[pair], send3.at[0, 0], recv3.at[pair], me).wait_recv()

    @pl.when(me == 0)
    def _():
        for copy in firsts:
            copy.wait_send()

    for slot in (1, 0):
        active = (place == 1) if slot else (place > 0)

        @pl.when(active & (block < far - 1))
        def _():
            outs[slot].wait_send()

        @pl.when(active & (block == far - 1))
        def _():
            @pl.loop(1, ring)
            def _(k):
                final_copy(slot, 0 if slot else place, k).wait_send()


def kernel(
    ring,
    heads,
    all_heads,
    x_hbm,
    wk_hbm,
    wv_hbm,
    wb_hbm,
    wf_hbm,
    speed_hbm,
    extra_hbm,
    probe_hbm,
    states_ref,
    reads_ref,
    speed_ref,
    extra_ref,
    probe_ref,
    x_ref,
    w_ref,
    wg_ref,
    gate_ref,
    raw_ref,
    pre_ref,
    low_ref,
    inside_ref,
    start_ref,
    right_ref,
    carried_ref,
    closing_ref,
    tiles,
    near_ref,
    sent_ref,
    far_ref,
    first_ref,
    rows_ref,
    final_ref,
    q_ref,
    gate_sems,
    w_sems,
    x_sems,
    send1,
    recv1,
    send2,
    recv2,
    send_first,
    recv_first,
    send3,
    recv3,
    ready,
):
    me = lax.axis_index("sp")
    width = heads * HEAD
    seqs, span, _ = x_hbm.shape
    pairs = heads // 2
    near = seqs * pairs
    far = ring // near
    barrier = pltpu.get_barrier_semaphore()
    gates = [
        pltpu.make_async_copy(wb_hbm, wg_ref.at[:all_heads], gate_sems.at[0]),
        pltpu.make_async_copy(wf_hbm, wg_ref.at[all_heads:], gate_sems.at[1]),
        pltpu.make_async_copy(extra_hbm, extra_ref, gate_sems.at[2]),
        pltpu.make_async_copy(probe_hbm, probe_ref, gate_sems.at[3]),
        pltpu.make_async_copy(speed_hbm, speed_ref, gate_sems.at[4]),
    ]
    depth = x_hbm.shape[2] // PIECES
    steps = span // ROWS
    first_pieces = []
    for k in range(PIECES):
        at = pl.ds(k * depth, depth)
        first_pieces.append([
            pltpu.make_async_copy(wk_hbm.at[at], w_ref.at[at, :width], w_sems.at[0, k]),
            pltpu.make_async_copy(wv_hbm.at[at], w_ref.at[at, width:], w_sems.at[1, k]),
            pltpu.make_async_copy(x_hbm.at[0, :ROWS, at], x_ref.at[:ROWS, at], w_sems.at[2, k]),
        ])
    later = []
    for step in range(1, seqs * steps):
        s, first = divmod(step * ROWS, span)
        later.append([
            pltpu.make_async_copy(
                x_hbm.at[s, pl.ds(first, ROWS)], x_ref.at[pl.ds(step * ROWS, ROWS)], x_sems.at[step]
            )
        ])
    queue = first_pieces + later
    for n, copies in enumerate(queue[:AHEAD]):
        for copy in copies:
            copy.start()
        if n == 0:
            for copy in gates:
                copy.start()
    greet(ring, near, me, barrier)

    def taken_in(k):
        def wait():
            for copy in queue[k]:
                copy.wait()
            for copies in queue[k + AHEAD : k + AHEAD + 1] if k + 1 < PIECES else queue[k + AHEAD :]:
                for copy in copies:
                    copy.start()

        return wait

    project(0, [taken_in(k) for k in range(PIECES)], x_ref, w_ref, raw_ref)
    met(ring, near, me, barrier, ready)

    for copy in gates:
        copy.wait()
    first = lax.axis_index("tp") * heads
    i, j = iotas((16, 2 * all_heads))
    taken = ((i < heads) & (j == first + i)) | ((i >= 8) & (i < 8 + heads) & (j == all_heads + first + i - 8))
    gate_ref[...] = dot(jnp.where(taken, 1.0, 0.0).astype(BF16), wg_ref[...]).astype(BF16)
    project_gates(0, x_ref, gate_ref, pre_ref)
    for s in range(seqs):
        for p in range(pairs):
            q_ref[s * pairs + p : s * pairs + p + 1, :] = probe_ref[s : s + 1, p * LANES : (p + 1) * LANES].astype(F32)
    parts = (low_ref, inside_ref, start_ref, right_ref, carried_ref, closing_ref)
    total = seqs * steps

    @pl.loop(1, total)
    def _(step):
        arrival = pltpu.make_async_copy(
            x_hbm.at[0, pl.ds(0, ROWS)], x_ref.at[pl.ds(step * ROWS, ROWS)], x_sems.at[step]
        )
        arrival.wait()
        chunk_parts(step - 1, heads, raw_ref, pre_ref, extra_ref, speed_ref, *parts)
        project(step, [], x_ref, w_ref, raw_ref)
        project_gates(step, x_ref, gate_ref, pre_ref)

    place, block = lax.rem(me, near), lax.div(me, near)

    def near_copy(pair):
        to, slot = max(pair, 1), int(pair == 0)
        return remote(
            tiles.at[pair], near_ref.at[slot, place], send1.at[pair], recv1.at[slot, place], block * near + to
        )

    chunks = span // CHUNK
    chunk_parts(total - 1, heads, raw_ref, pre_ref, extra_ref, speed_ref, *parts)
    state = small_inverses(0, chunks, heads, inside_ref, start_ref)
    for s in range(seqs):
        if s + 1 < seqs:
            following = small_inverses(s + 1, chunks, heads, inside_ref, start_ref)
            for slot, x in enumerate(following):
                inside_ref[(s + 1) * chunks * heads + slot] = x
        sequence_maps(s, chunks, heads, state, low_ref, right_ref, carried_ref, closing_ref, tiles)
        for p in range(pairs):
            pair = s * pairs + p

            @pl.when((me > 0) & (place != max(pair, 1)))
            def _():
                near_copy(pair).start()

        if s + 1 < seqs:
            state = [inside_ref[(s + 1) * chunks * heads + slot] for slot in range(chunks * heads)]

    exchange(
        ring, near, me, tiles, near_ref, sent_ref, far_ref, first_ref, rows_ref, final_ref, q_ref,
        (recv1, send2, recv2, send_first, recv_first, send3, recv3, ready),
    )
    for pair in range(near):
        @pl.when((me > 0) & (place != max(pair, 1)))
        def _():
            near_copy(pair).wait_send()

    rows = HEAD // ring
    _, lane = iotas((1, LANES))
    for s in range(seqs):
        for p in range(pairs):
            got = final_ref[s * pairs + p]
            states_ref[s, 2 * p] = got[:rows, :HEAD].astype(BF16)
            states_ref[s, 2 * p + 1] = swapped(got)[:rows, :HEAD].astype(BF16)
            read = got[rows : rows + 1]
            square = read * read
            even = jnp.sum(jnp.where(lane < HEAD, square, 0.0), axis=1, keepdims=True)
            odd = jnp.sum(jnp.where(lane < HEAD, 0.0, square), axis=1, keepdims=True)
            mean = jnp.where(lane < HEAD, even, odd) / HEAD
            reads_ref[s : s + 1, p * LANES : (p + 1) * LANES] = (read * lax.rsqrt(mean + 1e-06)).astype(BF16)


def body(
    ring,
    layer_feed,
    address_mapping,
    content_mapping,
    beta_mapping_matrix,
    forgetting_mapping,
    logged_fading_speed,
    extra_forgetting,
    opening_probe,
):
    seqs, span, depth = layer_feed.shape
    width = address_mapping.shape[1]
    heads = width // HEAD
    all_heads = beta_mapping_matrix.shape[1]
    tokens = seqs * span
    near = seqs * heads // 2
    chains = tokens // CHUNK * heads
    hbm = pl.BlockSpec(memory_space=pl.ANY)
    vmem = pl.BlockSpec(memory_space=pltpu.VMEM)
    dma = pltpu.SemaphoreType.DMA
    return pl.pallas_call(
        functools.partial(kernel, ring, heads, all_heads),
        out_shape=(
            jax.ShapeDtypeStruct((seqs, heads, HEAD // ring, HEAD), BF16),
            jax.ShapeDtypeStruct((seqs, width), BF16),
        ),
        in_specs=[hbm] * 8,
        out_specs=(vmem, vmem),
        scratch_shapes=[
            pltpu.SMEM((heads,), F32),
            pltpu.VMEM((seqs, heads, span), BF16),
            pltpu.VMEM((seqs, width), BF16),
            pltpu.VMEM((tokens, depth), BF16),
            pltpu.VMEM((depth, 2 * width), BF16),
            pltpu.VMEM((2 * all_heads, depth), BF16),
            pltpu.VMEM((16, depth), BF16),
            pltpu.VMEM((tokens, 2 * width), BF16),
            pltpu.VMEM((tokens // ROWS, 16, ROWS), F32),
            pltpu.VMEM((chains, CHUNK, CHUNK), BF16),
            pltpu.VMEM((chains, CHUNK, CHUNK), BF16),
            pltpu.VMEM((chains, SMALL, CHUNK), BF16),
            pltpu.VMEM((chains, CHUNK, CHUNK), BF16),
            pltpu.VMEM((chains, CHUNK, CHUNK), BF16),
            pltpu.VMEM((chains, LANES), F32),
            pltpu.VMEM((near, LANES, LANES), F32),
            pltpu.VMEM((2, near, LANES, LANES), F32),
            pltpu.VMEM((near, LANES, LANES), F32),
            pltpu.VMEM((2, ring // near - 1, LANES, LANES), F32),
            pltpu.VMEM((2, HEAD, LANES), F32),
            pltpu.VMEM((2, ring, 8, LANES), F32),
            pltpu.VMEM((near, 8, LANES), F32),
            pltpu.VMEM((near, LANES), F32),
            dma((5,)),
            dma((3, PIECES)),
            dma((tokens // ROWS,)),
            dma((near,)),
            dma((2, near)),
            dma((2,)),
            dma((2, ring // near - 1)),
            dma((near,)),
            dma((2,)),
            dma((2, ring)),
            dma((near,)),
            pltpu.SemaphoreType.REGULAR,
        ],
        compiler_params=pltpu.CompilerParams(
            collective_id=0, has_side_effects=True, vmem_limit_bytes=56 * 1024 * 1024
        ),
    )(
        layer_feed,
        address_mapping,
        content_mapping,
        beta_mapping_matrix.T,
        forgetting_mapping.T,
        logged_fading_speed,
        extra_forgetting.transpose(0, 2, 1),
        opening_probe,
    )


def solution(mesh):
    in_specs = (
        P("grp", "sp", None),
        P(None, "tp"),
        P(None, "tp"),
        P(),
        P(),
        P("tp"),
        P("grp", "sp", "tp"),
        P("grp", "tp"),
    )
    out_specs = (P("grp", "tp", "sp", None), P("grp", "tp"))
    return jax.shard_map(
        functools.partial(body, mesh.shape["sp"]),
        mesh=mesh,
        in_specs=in_specs,
        out_specs=out_specs,
        check_vma=False,
    )
```

```python
import functools

import jax
import jax.numpy as jnp
from jax import lax
from jax.experimental import pallas as pl
from jax.experimental.pallas import tpu as pltpu
from jax.sharding import PartitionSpec as P

HEAD = 64
LANES = 128
CHUNK = 128
ROWS = 256
PIECES = 4
AHEAD = 3
MESH = pl.DeviceIdType.MESH
F32 = jnp.float32
BF16 = jnp.bfloat16
NN = (((1,), (0,)), ((), ()))
NT = (((1,), (1,)), ((), ()))
TN = (((0,), (0,)), ((), ()))


def dot(left, right, dims=NN):
    return lax.dot_general(left, right, dims, preferred_element_type=F32)


def split(x):
    high = x.astype(BF16)
    return high, (x - high.astype(F32)).astype(BF16)


def matmul(left, right):
    lh, ll = split(left)
    rh, rl = split(right)
    wide = jnp.concatenate(
        [jnp.concatenate([rh, rl], axis=1), jnp.concatenate([rh, jnp.zeros_like(rh)], axis=1)], axis=0
    )
    both = dot(jnp.concatenate([lh, ll], axis=1), wide)
    return both[:, : right.shape[1]] + both[:, right.shape[1] :]


def iotas(shape):
    return lax.broadcasted_iota(jnp.int32, shape, 0), lax.broadcasted_iota(jnp.int32, shape, 1)


def swapped(x):
    return pltpu.roll(x, HEAD, 1)


def diagonal():
    i, j = iotas((LANES, LANES))
    return (i < HEAD) == (j < HEAD)


def composed(later, earlier):
    own = diagonal()
    return matmul(jnp.where(own, swapped(later), 0.0), earlier) + jnp.where(own, later, 0.0)


def silu(x):
    return x / (1.0 + jnp.exp(-x))


def project(step, pieces, x_ref, w_ref, raw_ref):
    rows = pl.ds(step * ROWS, ROWS)
    count = max(len(pieces), 1)
    depth = x_ref.shape[1] // count
    both = None
    for k in range(count):
        if pieces:
            pieces[k]()
        at = slice(k * depth, (k + 1) * depth)
        part = dot(x_ref[rows, at], w_ref[at, :])
        both = part if k == 0 else both + part
    raw_ref[rows, :] = both.astype(BF16)


def project_gates(step, x_ref, gate_ref, pre_ref):
    pre_ref[step] = dot(gate_ref[...], x_ref[pl.ds(step * ROWS, ROWS), :], NT).astype(BF16).astype(F32)


def chunk_parts(
    step, heads, raw_ref, pre_ref, extra_ref, speed_ref, low_ref, inside_ref, start_ref, right_ref, carried_ref, closing_ref
):
    rows = pl.ds(step * ROWS, ROWS)
    width = heads * HEAD
    keys = silu(raw_ref[rows, :width].astype(F32))
    i, j = iotas((width, width))
    same = jnp.where(i // HEAD == j // HEAD, 1.0, 0.0).astype(BF16)
    squares = dot((keys * keys).astype(BF16), same)
    keys = keys * lax.rsqrt(squares + 1e-06)
    values = silu(raw_ref[rows, width:].astype(F32))
    pre = pre_ref[step]

    spans = extra_ref.shape[2] // ROWS
    at = pl.ds(pl.multiple_of(lax.rem(step, spans) * ROWS, ROWS), ROWS)
    extra = extra_ref[lax.div(step, spans), :, at].astype(F32)
    extra = jnp.concatenate([extra, jnp.zeros((8 - heads, ROWS), F32)], axis=0)
    i, _ = iotas((8, ROWS))
    speed = jnp.zeros((8, ROWS), F32)
    for h in range(heads):
        speed = jnp.where(i == h, speed_ref[h], speed)
    betas = 1.0 / (1.0 + jnp.exp(-pre[:8]))
    fade = pre[8:]
    plus = jnp.maximum(fade, 0.0) + jnp.log(1.0 + jnp.exp(-jnp.abs(fade)))
    decay = -jnp.exp(speed) * plus + extra

    i, j = iotas((CHUNK, CHUNK))
    until = jnp.where(i <= j, 1.0, 0.0)
    left = j < HEAD
    left_bf = jnp.where(left, 1.0, 0.0).astype(BF16)
    near = jnp.where((i // SMALL) == (j // SMALL), 1.0, 0.0).astype(BF16)
    r, l = iotas((SMALL, LANES))
    c = l % SMALL
    close = jnp.where(r > c, r ^ c, 0)
    unit = jnp.where(r == c, 1.0, 0.0)
    for part in range(ROWS // CHUNK):
        at = slice(part * CHUNK, (part + 1) * CHUNK)
        totals = lax.dot_general(
            decay[:, at], until, NN, precision=lax.Precision.HIGHEST, preferred_element_type=F32
        )
        mixed = jnp.concatenate([betas[:, at], totals], axis=0)
        cols = jnp.transpose(mixed)
        for p in range(heads // 2):
            pair = slice(p * LANES, (p + 1) * LANES)
            k, v = keys[at, pair], values[at, pair]
            turned = swapped(k)
            kb = k.astype(BF16)
            even = kb * left_bf
            gram = dot(jnp.concatenate([even, kb - even], axis=0), kb, NT)
            for side in range(2):
                h = 2 * p + side
                slot = (step * (ROWS // CHUNK) + part) * heads + h
                mine = left if side == 0 else ~left
                beta = jnp.broadcast_to(cols[:, h : h + 1], (CHUNK, LANES))
                total = jnp.broadcast_to(cols[:, 8 + h : 9 + h], (CHUNK, LANES))
                ahead = jnp.broadcast_to(mixed[8 + h : 9 + h, :], (CHUNK, LANES))
                lower = beta * gram[side * CHUNK : (side + 1) * CHUNK] * jnp.exp(total - ahead)
                lower = jnp.where(i > j, lower, 0.0).astype(BF16)
                low_ref[slot] = lower
                inside = lower * near
                inside_ref[slot] = inside
                packed = inside[:SMALL]
                for b in range(1, CHUNK // SMALL):
                    packed = packed + inside[b * SMALL : (b + 1) * SMALL]
                start_ref[slot] = (unit - jnp.where(close == 1, packed.astype(F32), 0.0)).astype(BF16)
                right_ref[slot] = (beta * jnp.where(mine, v, -jnp.exp(total) * turned)).astype(BF16)
                last = total[CHUNK - 1 :, :]
                carried_ref[slot] = jnp.where(mine, k * jnp.exp(last - total), 0.0).astype(BF16)
                closing_ref[pl.ds(slot, 1), :] = jnp.exp(last)


SMALL = 16


def small_inverses(s, chunks, heads, inside_ref, start_ref):
    first = s * chunks * heads
    slots = range(chunks * heads)
    count = CHUNK // SMALL
    i, j = iotas((CHUNK, CHUNK))
    same = jnp.where((i // SMALL) == (j // SMALL), 1.0, 0.0).astype(BF16)
    r, l = iotas((SMALL, LANES))
    c = l % SMALL
    close = jnp.where(r > c, r ^ c, 0)

    def by_two(lefts, rights):
        out = []
        for n in range(0, len(lefts), 2):
            both = dot(jnp.concatenate(lefts[n : n + 2], axis=0), jnp.concatenate(rights[n : n + 2], axis=1))
            out += [both[:SMALL, :LANES], both[SMALL:, LANES:]]
        return out

    state = [start_ref[first + slot] for slot in slots]
    level = 1
    while 2 << level <= SMALL:
        inner = [y.astype(BF16) for y in by_two(state, [inside_ref[first + slot] for slot in slots])]
        inner = by_two(inner, [jnp.concatenate([x] * count, axis=0) * same for x in state])
        state = [x - jnp.where((close >> level) == 1, y, 0.0).astype(BF16) for x, y in zip(state, inner)]
        level += 1
    return [jnp.concatenate([x] * count, axis=0) * same for x in state]


def sequence_maps(s, chunks, heads, state, low_ref, right_ref, carried_ref, closing_ref, tiles):
    first = s * chunks * heads
    i, j = iotas((CHUNK, CHUNK))
    apart = jnp.where(i > j, i ^ j, 0)
    level = SMALL.bit_length() - 1
    while 2 << level <= CHUNK:
        size = 1 << level
        odd = [slice(b * size, (b + 1) * size) for b in range(1, CHUNK // size, 2)]
        even = [slice(b * size, (b + 1) * size) for b in range(0, CHUNK // size, 2)]
        here = jnp.concatenate([apart[at] for at in odd], axis=0)
        part = [jnp.concatenate([x[at] for at in odd], axis=0) for x in state]
        inner = [dot(x, low_ref[first + slot]).astype(BF16) for slot, x in enumerate(part)]
        inner = [dot(y, x) for y, x in zip(inner, state)]
        part = [x - jnp.where((here >> level) == 1, y, 0.0).astype(BF16) for x, y in zip(part, inner)]
        state = [
            jnp.concatenate(
                [z for b, at in enumerate(even) for z in (x[at], y[b * size : (b + 1) * size])], axis=0
            )
            for x, y in zip(state, part)
        ]
        level += 1
    solved = [dot(x, right_ref[first + slot]).astype(BF16) for slot, x in enumerate(state)]
    for p in range(heads // 2):
        parts = []
        for n in range(chunks):
            slot = n * heads + 2 * p
            carried = jnp.concatenate([carried_ref[first + slot], carried_ref[first + slot + 1]], axis=0)
            tile = dot(carried, jnp.concatenate(solved[slot : slot + 2], axis=0), TN)
            closing = [
                jnp.broadcast_to(closing_ref[pl.ds(first + slot + side, 1), :], tile.shape) for side in range(2)
            ]
            parts.append(tile + jnp.where(j == (i ^ HEAD), jnp.where(i < HEAD, *closing), 0.0))
        while len(parts) > 1:
            parts = [composed(parts[n + 1], parts[n]) for n in range(0, len(parts), 2)]
        tiles[s * (heads // 2) + p] = parts[0]


def remote(src, dst, send, recv, to):
    return pltpu.make_async_remote_copy(
        src_ref=src, dst_ref=dst, send_sem=send, recv_sem=recv, device_id={"sp": to}, device_id_type=MESH
    )


def signal(semaphore, to):
    pl.semaphore_signal(semaphore, inc=1, device_id={"sp": to}, device_id_type=MESH)


def greet(ring, near, me, barrier):
    far = ring // near
    place, block = lax.rem(me, near), lax.div(me, near)
    for k in range(1, near):
        to = block * near + lax.rem(place + k, near)

        @pl.when((me > 0) & (to > 0))
        def _():
            signal(barrier, to)

    @pl.when(block < far - 1)
    def _():
        for k in range(near):
            signal(barrier, (far - 1) * near + k)


def met(ring, near, me, barrier, ready):
    far = ring // near
    place, block = lax.rem(me, near), lax.div(me, near)
    count = jnp.where(block == far - 1, ring - 1, jnp.where(block == 0, near - 2, near - 1))

    @pl.when(me > 0)
    def _():
        pl.semaphore_wait(barrier, count)

    @pl.when((block == far - 1) & (place > 0))
    def _():
        signal(ready, 0)
        for b in range(far - 1):
            signal(ready, b * near + place)


def exchange(ring, near, me, tiles, near_ref, sent_ref, far_ref, first_ref, rows_ref, final_ref, probe_ref, sems):
    recv1, send2, recv2, send_first, recv_first, send3, recv3, ready = sems
    far = ring // near
    place, block = lax.rem(me, near), lax.div(me, near)
    own = diagonal()
    i, j = iotas((LANES, LANES))

    firsts = []
    for pair in range(near):
        to, slot = max(pair, 1), int(pair == 0)
        firsts.append(
            remote(
                sent_ref.at[pair, :HEAD], first_ref.at[slot], send_first.at[pair], recv_first.at[slot],
                (far - 1) * near + to,
            )
        )

    @pl.when(me == 0)
    def _():
        for pair in range(near):
            tile = jnp.where(own, tiles[pair], 0.0)
            sent_ref[pair, :HEAD] = tile[:HEAD] + tile[HEAD:]
        pl.semaphore_wait(ready, near - 1)
        for copy in firsts:
            copy.start()

    outs = [
        remote(
            sent_ref.at[slot], far_ref.at[slot, jnp.minimum(block, far - 2)], send2.at[slot],
            recv2.at[slot, jnp.minimum(block, far - 2)], (far - 1) * near + place,
        )
        for slot in range(2)
    ]

    def final_copy(slot, pair, k):
        to = lax.rem(me + k, ring)
        return remote(rows_ref.at[slot, to], final_ref.at[pair], send3.at[slot, k], recv3.at[pair], to)

    @pl.when((block < far - 1) & (place > 0))
    def _():
        pl.semaphore_wait(ready, 1)

    for slot in (1, 0):
        pair = 0 if slot else place

        @pl.when((place == 1) if slot else (place > 0))
        def _():
            near_ref[slot, place] = tiles[pair]

            @pl.when(block == 0)
            def _():
                near_ref[slot, 0] = jnp.where(j == (i ^ HEAD), 1.0, 0.0)

            def arrived(k):
                @pl.when((place != k) & ((block > 0) | (k > 0)))
                def _():
                    remote(tiles.at[0], near_ref.at[slot, k], send2.at[0], recv1.at[slot, k], me).wait_recv()

            arrived(0)
            tile = near_ref[slot, 0]
            for k in range(1, near):
                arrived(k)
                tile = composed(near_ref[slot, k], tile)

            @pl.when(block < far - 1)
            def _():
                sent_ref[slot] = tile
                outs[slot].start()

            @pl.when(block == far - 1)
            def _():
                remote(sent_ref.at[0, :HEAD], first_ref.at[slot], send2.at[0], recv_first.at[slot], me).wait_recv()
                state = first_ref[slot]
                state = jnp.where(own, jnp.concatenate([state, state], axis=0), 0.0)
                for b in range(far - 1):
                    remote(sent_ref.at[0], far_ref.at[slot, b], send2.at[0], recv2.at[slot, b], me).wait_recv()
                    state = composed(far_ref[slot, b], state)
                state = jnp.where(own, composed(tile, state), 0.0)
                both = state[:HEAD] + state[HEAD:]
                rows = HEAD // ring
                read = matmul(jnp.broadcast_to(probe_ref[pl.ds(pair, 1), :], (8, LANES)), state)
                for d in range(ring):
                    rows_ref[slot, d, :rows] = both[d * rows : (d + 1) * rows]
                    rows_ref[slot, d, rows : rows + 1] = read[:1]

                @pl.loop(1, ring)
                def _(k):
                    final_copy(slot, pair, k).start()

                final_ref[pair] = rows_ref[slot, me]

    for pair in range(near):
        @pl.when((block < far - 1) | (place != max(pair, 1)))
        def _():
            remote(rows_ref.at[0, 0], final_ref.at[pair], send3.at[0, 0], recv3.at[pair], me).wait_recv()

    @pl.when(me == 0)
    def _():
        for copy in firsts:
            copy.wait_send()

    for slot in (1, 0):
        active = (place == 1) if slot else (place > 0)

        @pl.when(active & (block < far - 1))
        def _():
            outs[slot].wait_send()

        @pl.when(active & (block == far - 1))
        def _():
            @pl.loop(1, ring)
            def _(k):
                final_copy(slot, 0 if slot else place, k).wait_send()


def kernel(
    ring,
    heads,
    all_heads,
    x_hbm,
    wk_hbm,
    wv_hbm,
    wb_hbm,
    wf_hbm,
    speed_hbm,
    extra_hbm,
    probe_hbm,
    final_ref,
    speed_ref,
    extra_ref,
    probe_ref,
    x_ref,
    w_ref,
    wg_ref,
    gate_ref,
    raw_ref,
    pre_ref,
    low_ref,
    inside_ref,
    start_ref,
    right_ref,
    carried_ref,
    closing_ref,
    tiles,
    near_ref,
    sent_ref,
    far_ref,
    first_ref,
    rows_ref,
    q_ref,
    gate_sems,
    w_sems,
    x_sems,
    send1,
    recv1,
    send2,
    recv2,
    send_first,
    recv_first,
    send3,
    recv3,
    ready,
):
    me = lax.axis_index("sp")
    width = heads * HEAD
    seqs, span, _ = x_hbm.shape
    pairs = heads // 2
    near = seqs * pairs
    far = ring // near
    barrier = pltpu.get_barrier_semaphore()
    gates = [
        pltpu.make_async_copy(wb_hbm, wg_ref.at[:all_heads], gate_sems.at[0]),
        pltpu.make_async_copy(wf_hbm, wg_ref.at[all_heads:], gate_sems.at[1]),
        pltpu.make_async_copy(extra_hbm, extra_ref, gate_sems.at[2]),
        pltpu.make_async_copy(probe_hbm, probe_ref, gate_sems.at[3]),
        pltpu.make_async_copy(speed_hbm, speed_ref, gate_sems.at[4]),
    ]
    depth = x_hbm.shape[2] // PIECES
    steps = span // ROWS
    first_pieces = []
    for k in range(PIECES):
        at = pl.ds(k * depth, depth)
        first_pieces.append([
            pltpu.make_async_copy(wk_hbm.at[at], w_ref.at[at, :width], w_sems.at[0, k]),
            pltpu.make_async_copy(wv_hbm.at[at], w_ref.at[at, width:], w_sems.at[1, k]),
            pltpu.make_async_copy(x_hbm.at[0, :ROWS, at], x_ref.at[:ROWS, at], w_sems.at[2, k]),
        ])
    later = []
    for step in range(1, seqs * steps):
        s, first = divmod(step * ROWS, span)
        later.append([
            pltpu.make_async_copy(
                x_hbm.at[s, pl.ds(first, ROWS)], x_ref.at[pl.ds(step * ROWS, ROWS)], x_sems.at[step]
            )
        ])
    queue = first_pieces + later
    for n, copies in enumerate(queue[:AHEAD]):
        for copy in copies:
            copy.start()
        if n == 0:
            for copy in gates:
                copy.start()
    greet(ring, near, me, barrier)

    def taken_in(k):
        def wait():
            for copy in queue[k]:
                copy.wait()
            for copies in queue[k + AHEAD : k + AHEAD + 1] if k + 1 < PIECES else queue[k + AHEAD :]:
                for copy in copies:
                    copy.start()

        return wait

    project(0, [taken_in(k) for k in range(PIECES)], x_ref, w_ref, raw_ref)
    met(ring, near, me, barrier, ready)

    for copy in gates:
        copy.wait()
    first = lax.axis_index("tp") * heads
    i, j = iotas((16, 2 * all_heads))
    taken = ((i < heads) & (j == first + i)) | ((i >= 8) & (i < 8 + heads) & (j == all_heads + first + i - 8))
    gate_ref[...] = dot(jnp.where(taken, 1.0, 0.0).astype(BF16), wg_ref[...]).astype(BF16)
    project_gates(0, x_ref, gate_ref, pre_ref)
    for s in range(seqs):
        for p in range(pairs):
            q_ref[s * pairs + p : s * pairs + p + 1, :] = probe_ref[s : s + 1, p * LANES : (p + 1) * LANES].astype(F32)
    parts = (low_ref, inside_ref, start_ref, right_ref, carried_ref, closing_ref)
    total = seqs * steps

    @pl.loop(1, total)
    def _(step):
        arrival = pltpu.make_async_copy(
            x_hbm.at[0, pl.ds(0, ROWS)], x_ref.at[pl.ds(step * ROWS, ROWS)], x_sems.at[step]
        )
        arrival.wait()
        chunk_parts(step - 1, heads, raw_ref, pre_ref, extra_ref, speed_ref, *parts)
        project(step, [], x_ref, w_ref, raw_ref)
        project_gates(step, x_ref, gate_ref, pre_ref)

    place, block = lax.rem(me, near), lax.div(me, near)

    def near_copy(pair):
        to, slot = max(pair, 1), int(pair == 0)
        return remote(
            tiles.at[pair], near_ref.at[slot, place], send1.at[pair], recv1.at[slot, place], block * near + to
        )

    chunks = span // CHUNK
    chunk_parts(total - 1, heads, raw_ref, pre_ref, extra_ref, speed_ref, *parts)
    state = small_inverses(0, chunks, heads, inside_ref, start_ref)
    for s in range(seqs):
        if s + 1 < seqs:
            following = small_inverses(s + 1, chunks, heads, inside_ref, start_ref)
            for slot, x in enumerate(following):
                inside_ref[(s + 1) * chunks * heads + slot] = x
        sequence_maps(s, chunks, heads, state, low_ref, right_ref, carried_ref, closing_ref, tiles)
        for p in range(pairs):
            pair = s * pairs + p

            @pl.when((me > 0) & (place != max(pair, 1)))
            def _():
                near_copy(pair).start()

        if s + 1 < seqs:
            state = [inside_ref[(s + 1) * chunks * heads + slot] for slot in range(chunks * heads)]

    exchange(
        ring, near, me, tiles, near_ref, sent_ref, far_ref, first_ref, rows_ref, final_ref, q_ref,
        (recv1, send2, recv2, send_first, recv_first, send3, recv3, ready),
    )
    for pair in range(near):
        @pl.when((me > 0) & (place != max(pair, 1)))
        def _():
            near_copy(pair).wait_send()


def finish(ring, final_ref, states_ref, reads_ref):
    seqs, heads = states_ref.shape[:2]
    pairs = heads // 2
    rows = HEAD // ring
    _, lane = iotas((1, LANES))
    for s in range(seqs):
        for p in range(pairs):
            got = final_ref[s * pairs + p]
            states_ref[s, 2 * p] = got[:rows, :HEAD].astype(BF16)
            states_ref[s, 2 * p + 1] = swapped(got)[:rows, :HEAD].astype(BF16)
            read = got[rows : rows + 1]
            square = read * read
            even = jnp.sum(jnp.where(lane < HEAD, square, 0.0), axis=1, keepdims=True)
            odd = jnp.sum(jnp.where(lane < HEAD, 0.0, square), axis=1, keepdims=True)
            mean = jnp.where(lane < HEAD, even, odd) / HEAD
            reads_ref[s : s + 1, p * LANES : (p + 1) * LANES] = (read * lax.rsqrt(mean + 1e-06)).astype(BF16)


def body(
    ring,
    layer_feed,
    address_mapping,
    content_mapping,
    beta_mapping_matrix,
    forgetting_mapping,
    logged_fading_speed,
    extra_forgetting,
    opening_probe,
):
    seqs, span, depth = layer_feed.shape
    width = address_mapping.shape[1]
    heads = width // HEAD
    all_heads = beta_mapping_matrix.shape[1]
    tokens = seqs * span
    near = seqs * heads // 2
    chains = tokens // CHUNK * heads
    hbm = pl.BlockSpec(memory_space=pl.ANY)
    vmem = pl.BlockSpec(memory_space=pltpu.VMEM)
    dma = pltpu.SemaphoreType.DMA
    final = pl.pallas_call(
        functools.partial(kernel, ring, heads, all_heads),
        out_shape=jax.ShapeDtypeStruct((near, 8, LANES), F32),
        in_specs=[hbm] * 8,
        out_specs=vmem,
        scratch_shapes=[
            pltpu.SMEM((heads,), F32),
            pltpu.VMEM((seqs, heads, span), BF16),
            pltpu.VMEM((seqs, width), BF16),
            pltpu.VMEM((tokens, depth), BF16),
            pltpu.VMEM((depth, 2 * width), BF16),
            pltpu.VMEM((2 * all_heads, depth), BF16),
            pltpu.VMEM((16, depth), BF16),
            pltpu.VMEM((tokens, 2 * width), BF16),
            pltpu.VMEM((tokens // ROWS, 16, ROWS), F32),
            pltpu.VMEM((chains, CHUNK, CHUNK), BF16),
            pltpu.VMEM((chains, CHUNK, CHUNK), BF16),
            pltpu.VMEM((chains, SMALL, CHUNK), BF16),
            pltpu.VMEM((chains, CHUNK, CHUNK), BF16),
            pltpu.VMEM((chains, CHUNK, CHUNK), BF16),
            pltpu.VMEM((chains, LANES), F32),
            pltpu.VMEM((near, LANES, LANES), F32),
            pltpu.VMEM((2, near, LANES, LANES), F32),
            pltpu.VMEM((near, LANES, LANES), F32),
            pltpu.VMEM((2, ring // near - 1, LANES, LANES), F32),
            pltpu.VMEM((2, HEAD, LANES), F32),
            pltpu.VMEM((2, ring, 8, LANES), F32),
            pltpu.VMEM((near, LANES), F32),
            dma((5,)),
            dma((3, PIECES)),
            dma((tokens // ROWS,)),
            dma((near,)),
            dma((2, near)),
            dma((2,)),
            dma((2, ring // near - 1)),
            dma((near,)),
            dma((2,)),
            dma((2, ring)),
            dma((near,)),
            pltpu.SemaphoreType.REGULAR,
        ],
        compiler_params=pltpu.CompilerParams(
            collective_id=0, has_side_effects=True, vmem_limit_bytes=56 * 1024 * 1024
        ),
    )(
        layer_feed,
        address_mapping,
        content_mapping,
        beta_mapping_matrix.T,
        forgetting_mapping.T,
        logged_fading_speed,
        extra_forgetting.transpose(0, 2, 1),
        opening_probe,
    )
    return pl.pallas_call(
        functools.partial(finish, ring),
        out_shape=(
            jax.ShapeDtypeStruct((seqs, heads, HEAD // ring, HEAD), BF16),
            jax.ShapeDtypeStruct((seqs, width), BF16),
        ),
        in_specs=[vmem],
        out_specs=(vmem, vmem),
    )(final)


def solution(mesh):
    in_specs = (
        P("grp", "sp", None),
        P(None, "tp"),
        P(None, "tp"),
        P(),
        P(),
        P("tp"),
        P("grp", "sp", "tp"),
        P("grp", "tp"),
    )
    out_specs = (P("grp", "tp", "sp", None), P("grp", "tp"))
    return jax.shard_map(
        functools.partial(body, mesh.shape["sp"]),
        mesh=mesh,
        in_specs=in_specs,
        out_specs=out_specs,
        check_vma=False,
    )
```
